256 devices in a mesh: ep: 64 (over z, x, core), tp: 4 (over y).
Axes of the slice: x: 4, y: 4, z: 8, core: 2. Of those that a mesh axis runs over, the one named last changes fastest.
Arguments:
- receptance: bfloat16 [32768, 2048], P('ep', 'tp'), may hold values from -6 to 6
- key_rows: bfloat16 [32768, 2048], P('ep', 'tp'), may hold values from -6 to 6
- value_rows: bfloat16 [32768, 2048], P('ep', 'tp'), may hold values from -6 to 6
- decay_input: bfloat16 [32768, 2048], P('ep', 'tp'), may hold values from -2.796875 to 2.796875
- learn_input: bfloat16 [32768, 2048], P('ep', 'tp'), may hold values from -12 to 4
- decay_base: float32 [2048], P('tp'), may hold values from -20 to -2
- decay_shift: float32 [32768, 32], P('ep', 'tp'), may hold values from -1 to 20
- channel_gain: float32 [2048], P('tp'), may hold values from 0.1 to 1.9
- out_weight: bfloat16 [2048, 2048], P('tp'), may hold values from -0.125 to 0.125
- expert_input: bfloat16 [32768, 2048], P(('ep', 'tp')), may hold values from -6 to 6
- expert_gain: float32 [2048], replicated, may hold values from 0.1 to 1.9
- routes: int32 [32768, 2], P(('ep', 'tp')), may hold values from 0 to 63, all different within a row; in each aligned block of 128 rows (0 to 127, 128 to 255, ...) at most 8 rows name the same one
- route_weight: float32 [32768, 2], P(('ep', 'tp')), may hold values from 0.1 to 1
- gate_weight: bfloat16 [64, 2048, 1024], P('ep', None, 'tp'), may hold values from -0.125 to 0.125
- up_weight: bfloat16 [64, 2048, 1024], P('ep', None, 'tp'), may hold values from -0.125 to 0.125
- down_weight: bfloat16 [64, 1024, 2048], P('ep', 'tp'), may hold values from -0.1875 to 0.1875
Outputs:
- mixer_out: bfloat16 [32768, 2048], P(('ep', 'tp'))
- expert_out: bfloat16 [32768, 2048], P(('ep', 'tp'))
The draws below stay inside these ranges and needn't reach their ends.
Inputs may be any that keep to these rules, and one draw needn't show every extreme that they name: `routes`: within the rows of one device (aligned blocks of 128 rows) no expert is named by more than 8 rows, and in every draw some block names some expert exactly 8 times. Each row names 2 different experts.
All inputs are finite; a program needn't handle non-finite values.
Results may differ from the reference program's by a relative error of at most 0.024.
Values may be sent and summed in bfloat16 or wider, within the bound.
A program may use at most 128 MiB of HBM per device.

```python
import math
import jax
import jax.numpy as jnp
import numpy as np
from jax import lax

D = 2048
HEADS = 32
HEAD = 64
CHANNELS = 2048
FF = 1024
EXPERTS = 64
TOPK = 2
TOK_DEV = 128
MIX_ROWS = 512
MICRO_TOKENS = 32768
CAP = 8
N_TP = 4


def fast_heads(key):
    ranking = jax.random.permutation(jax.random.fold_in(key, 101), HEADS)
    quick_count = HEADS // 2
    return jnp.repeat(ranking < quick_count, HEAD)


def draw_decay_base(key, part):
    quick = fast_heads(key)
    spread = jax.random.uniform(jax.random.fold_in(key, 102), (CHANNELS,), jnp.float32)
    slow_rates = -jnp.log(jnp.float32(MICRO_TOKENS)) - 2.0 - spread
    quick_rates = -3.9 + 1.3 * spread
    return jnp.where(quick, quick_rates, slow_rates).astype(jnp.float32)


def draw_decay_shift(key, part):
    blocks = MICRO_TOKENS // MIX_ROWS
    reach = 0.5
    levels = jax.random.uniform(jax.random.fold_in(key, 103), (blocks, HEADS), jnp.float32, -reach, reach)
    each_row_amount = jnp.repeat(levels, MIX_ROWS, axis=0)
    surge_locations = jax.random.randint(jax.random.fold_in(key, 104), (3,), 0, MICRO_TOKENS)
    surge_groups = jnp.any(jnp.arange(MICRO_TOKENS, dtype=jnp.int32)[:, None] == surge_locations[None, :], axis=1)
    table_height = jnp.log(jnp.float32(MICRO_TOKENS)) + 3.0
    return (each_row_amount + jnp.where(surge_groups, table_height, 0.0)[:, None]).astype(jnp.float32)


def draw_learn_input(key, part):
    quick = fast_heads(key)
    slow_mean = -jnp.log(jnp.float32(MICRO_TOKENS) / HEAD) - 1.0
    centre = jnp.where(quick, 0.0, slow_mean)
    jitter = jnp.clip(jax.random.normal(jax.random.fold_in(key, 105), (MICRO_TOKENS, CHANNELS), jnp.float32), -3.0, 3.0)
    return (centre[None, :] + jitter).astype(jnp.bfloat16)


def block_scale(own_key, shape, cuts, smallest, top_value):
    factor_of = 1.0
    for dim, shards_of in cuts:
        draws = jax.random.uniform(jax.random.fold_in(jax.random.fold_in(own_key, 6), dim), (shards_of,), jnp.float32, smallest / len(cuts), top_value / len(cuts))
        factor_of = factor_of * jnp.repeat(jnp.exp(draws), shape[dim] // shards_of).reshape((-1,) + (1,) * (len(shape) - 1 - dim))
    return factor_of


def assign_block(own_key, own, number, rows, count, top, most, lean):
    sequence = jax.random.permutation(own_key, count)
    packed, ordinary = load_shares(count, rows * top, most, lean, True), load_shares(count, rows * top, most, lean, False)
    places = jnp.arange(count)

    def named(lengths, turn):
        used = int((lengths > 0).sum())
        fixed = max(1, used // 4)
        shifted = fixed + (places - fixed + turn * (used - fixed)) % max(1, count - fixed)
        return jnp.zeros((count,), jnp.int32).at[sequence[jnp.where(places < fixed, places, shifted)]].set(jnp.asarray(lengths, jnp.int32))

    lengths = jnp.where(number % 4 == 0, named(packed, number // 4), named(ordinary, number - number // 4 - 1))
    mixed = jax.random.permutation(jax.random.fold_in(own, 3), count)
    giver, sink = mixed[0:count // 2 * 2:2], mixed[1:count // 2 * 2:2]
    slack = jnp.minimum(lengths[giver] - 1, most - lengths[sink]) // 2
    slack = jnp.where((giver == sequence[0]) | (sink == sequence[0]) | (lengths[sink] == 0), 0, jnp.maximum(slack, 0))
    shifted = jax.random.randint(jax.random.fold_in(own, 4), (count // 2,), 0, 1 << 20) % (slack + 1)
    lengths = lengths.at[giver].add(-shifted).at[sink].add(shifted)
    items = jnp.searchsorted(jnp.cumsum(lengths), jnp.arange(rows * top), side="right").astype(jnp.int32)
    listing = items.reshape(top, rows).T
    listing = listing[jax.random.permutation(jax.random.fold_in(own, 1), rows)]
    turn = jax.random.randint(jax.random.fold_in(own, 2), (rows, 1), 0, top)
    return jnp.take_along_axis(listing, (jnp.arange(top)[None, :] + turn) % top, axis=1)


def load_shares(number_of, total, most, lean, full):
    loads = [(1 << 20) // math.isqrt(grade ** lean) + 1 for grade in range(1, number_of + 1)]
    largest = most if full else min(most, max(-(-total // number_of), total * loads[0] // sum(loads)))
    least = 1 if total - largest >= number_of - 1 else 0
    given, rest = [largest] + [least] * (number_of - 1), total - largest - least * (number_of - 1)
    while rest > 0:
        free = [i for i in range(1, number_of) if given[i] < largest] or [i for i in range(1, number_of) if given[i] < most]
        mass, left = sum([loads[i] for i in free]), rest
        for i in free:
            addition = min(most - given[i], max(1, left * loads[i] // mass), rest)
            given[i] = given[i] + addition
            rest = rest - addition
    return np.array(given)


def noise(own_key, dims, deviation, limit, pieces=(), held_as=jnp.bfloat16):
    entries = deviation * jax.random.normal(own_key, dims, jnp.float32)
    if pieces:
        entries = entries * block_scale(own_key, dims, pieces, -0.22, 0.18)
    return jnp.clip(entries, -limit, limit).astype(held_as)


def setup_inputs(seed: int = 0) -> dict:
    key_list = jax.random.split(jax.random.key(seed), 17)
    receptance = noise(key_list[0], (MICRO_TOKENS, CHANNELS), 1.0, 6.0, ((0, 64), (1, 4)))
    key_rows = noise(key_list[1], (MICRO_TOKENS, CHANNELS), 1.0, 6.0, ((0, 64), (1, 4)))
    value_rows = noise(key_list[2], (MICRO_TOKENS, CHANNELS), 1.0, 6.0, ((0, 64), (1, 4)))
    decay_input = noise(key_list[3], (MICRO_TOKENS, CHANNELS), 0.7, 2.796875, ((0, 64), (1, 4)))
    learn_input = draw_learn_input(jax.random.fold_in(key_list[16], 71), 0)
    decay_base = draw_decay_base(jax.random.fold_in(key_list[16], 71), 0)
    decay_shift = draw_decay_shift(jax.random.fold_in(key_list[16], 71), 0)
    channel_gain = jnp.clip(1.0 + 0.18 * jax.random.normal(key_list[7], (CHANNELS,), jnp.float32), 0.1, 1.9)
    out_weight = noise(key_list[8], (CHANNELS, D), CHANNELS ** -0.5, 0.125, ((0, 4),))
    expert_input = noise(key_list[9], (MICRO_TOKENS, D), 1.0, 6.0, ((0, 256),))
    expert_gain = jnp.clip(1.0 + 0.18 * jax.random.normal(key_list[10], (D,), jnp.float32), 0.1, 1.9)
    routes_keys = jax.random.split(jax.random.fold_in(key_list[11], 1), MICRO_TOKENS // TOK_DEV)
    routes_turns = jax.random.permutation(jax.random.fold_in(key_list[11], 3), MICRO_TOKENS // TOK_DEV)
    routes = jax.vmap(lambda own, number: assign_block(jax.random.fold_in(key_list[11], 2), own, number, TOK_DEV, EXPERTS, TOPK, CAP, 1))(routes_keys, routes_turns).reshape((MICRO_TOKENS, TOPK))
    route_weight = jnp.clip(jnp.exp(math.log(1.0) - 2.3025851 * jax.random.uniform(key_list[12], (MICRO_TOKENS, TOPK), jnp.float32) ** block_scale(key_list[12], (MICRO_TOKENS, TOPK), ((0, 256),), -0.2, 0.2)), 0.1, 1.0)
    gate_weight = noise(key_list[13], (EXPERTS, D, FF), D ** -0.5, 0.125, ((0, 64), (2, 4)))
    up_weight = noise(key_list[14], (EXPERTS, D, FF), D ** -0.5, 0.125, ((0, 64), (2, 4)))
    down_weight = noise(key_list[15], (EXPERTS, FF, D), FF ** -0.5, 0.1875, ((0, 64), (1, 4)))
    return {"receptance": receptance, "key_rows": key_rows, "value_rows": value_rows, "decay_input": decay_input, "learn_input": learn_input, "decay_base": decay_base, "decay_shift": decay_shift, "channel_gain": channel_gain, "out_weight": out_weight, "expert_input": expert_input, "expert_gain": expert_gain, "routes": routes, "route_weight": route_weight, "gate_weight": gate_weight, "up_weight": up_weight, "down_weight": down_weight}


NORM_EPS = 1e-06
GROUP_EPS = 0.00064
KEY_EPS = 1e-06
PRECISE = lax.Precision.HIGHEST

def rounded_sum(inputs, weight, groups):
    group_size = inputs.shape[1] // groups
    result = jnp.zeros((inputs.shape[0], weight.shape[1]), jnp.float32)
    for part_index in range(groups):
        lower = part_index * group_size
        partial_value = jnp.dot(inputs[:, lower:lower + group_size], weight[lower:lower + group_size], preferred_element_type=jnp.float32)
        result = result + lax.optimization_barrier(partial_value.astype(jnp.bfloat16)).astype(jnp.float32)
    return result.astype(jnp.bfloat16)

def slot_targets(block_routes, experts, capacity):
    flat_routes = block_routes.reshape(-1)
    matches = (flat_routes[:, None] == jnp.arange(experts, dtype=jnp.int32)[None, :]).astype(jnp.int32)
    earlier = jnp.cumsum(matches, axis=0) - matches
    slots = lax.optimization_barrier(jnp.sum(earlier * matches, axis=1)).reshape(block_routes.shape)
    return (block_routes * capacity + slots).astype(jnp.int32)

def token_mixer(receptance, key_rows, value_rows, decay_input, learn_input, decay_base, decay_shift, channel_gain, out_weight):
    head_shape = (MICRO_TOKENS, HEADS, HEAD)
    recept = receptance.astype(jnp.float32).reshape(head_shape)
    key_data = key_rows.astype(jnp.float32).reshape(head_shape)
    value_data = value_rows.astype(jnp.float32).reshape(head_shape)
    pre_decay = decay_input.astype(jnp.float32).reshape(head_shape) + decay_base.reshape(1, HEADS, HEAD) + decay_shift[:, :, None]
    decays = jnp.exp(-jnp.exp(-jax.nn.softplus(-pre_decay) - 0.5))
    rates = jax.nn.sigmoid(learn_input.astype(jnp.float32)).reshape(head_shape)
    unit_keys = key_data / jnp.sqrt(lax.optimization_barrier(jnp.sum(key_data * key_data, axis=2, keepdims=True)) + KEY_EPS)
    removal = unit_keys * rates

    def advance(state, inputs):
        recept_now, decay_now, key_now, value_now, unit_now, removal_now = inputs
        probes = jnp.einsum('hij,hj->hi', state, unit_now, precision=PRECISE)
        state = state * decay_now[:, None, :] - probes[:, :, None] * removal_now[:, None, :] + value_now[:, :, None] * key_now[:, None, :]
        return (state, jnp.einsum('hij,hj->hi', state, recept_now, precision=PRECISE))
    start_state = jnp.zeros((HEADS, HEAD, HEAD), jnp.float32)
    _, readout = lax.scan(advance, start_state, (recept, decays, key_data, value_data, unit_keys, removal))
    centred = readout - lax.optimization_barrier(jnp.mean(readout, axis=2, keepdims=True))
    variance = lax.optimization_barrier(jnp.mean(centred * centred, axis=2, keepdims=True))
    normed = (centred * lax.rsqrt(variance + GROUP_EPS)).reshape(MICRO_TOKENS, CHANNELS) * channel_gain
    return rounded_sum(normed.astype(jnp.bfloat16), out_weight, N_TP)

def expert_layer(expert_input, expert_gain, routes, route_weight, gate_weight, up_weight, down_weight):
    inputs = expert_input.astype(jnp.float32)
    normed = (inputs * lax.rsqrt(lax.optimization_barrier(jnp.mean(inputs * inputs, axis=1, keepdims=True)) + NORM_EPS) * expert_gain).astype(jnp.bfloat16)
    blocks = MICRO_TOKENS // TOK_DEV
    block_routes = routes.reshape(blocks, TOK_DEV, TOPK)
    targets = jax.vmap(lambda member: slot_targets(member, EXPERTS, CAP))(block_routes)
    slots = targets - block_routes * CAP
    block_index = jnp.arange(blocks, dtype=jnp.int32)[:, None, None]
    places = ((block_routes * blocks + block_index) * CAP + slots).astype(jnp.int32)
    token_index = jnp.broadcast_to(jnp.arange(MICRO_TOKENS, dtype=jnp.int32).reshape(blocks, TOK_DEV, 1), places.shape)
    owners = jnp.full((EXPERTS * blocks * CAP,), MICRO_TOKENS, jnp.int32).at[places.reshape(-1)].set(token_index.reshape(-1))
    padded = jnp.concatenate([normed, jnp.zeros((1, D), jnp.bfloat16)], axis=0)

    def run_expert(operands):
        owner_rows, w_gate, w_up, w_down = operands
        gathered = padded[owner_rows]
        gates = jnp.dot(gathered, w_gate, preferred_element_type=jnp.float32)
        uppers = jnp.dot(gathered, w_up, preferred_element_type=jnp.float32)
        hidden = (jax.nn.silu(gates) * uppers).astype(jnp.bfloat16)
        return rounded_sum(hidden, w_down, N_TP)
    outputs = lax.map(run_expert, (owners.reshape(EXPERTS, blocks * CAP), gate_weight, up_weight, down_weight))
    flat_rows = outputs.reshape(EXPERTS * blocks * CAP, D)
    picks = places.reshape(MICRO_TOKENS, TOPK)
    combined = jnp.zeros((MICRO_TOKENS, D), jnp.float32)
    for picked in range(TOPK):
        combined = combined + flat_rows[picks[:, picked]].astype(jnp.float32) * route_weight[:, picked:picked + 1]
    return combined.astype(jnp.bfloat16)

def reference(receptance, key_rows, value_rows, decay_input, learn_input, decay_base, decay_shift, channel_gain, out_weight, expert_input, expert_gain, routes, route_weight, gate_weight, up_weight, down_weight):
    mixer_out = token_mixer(receptance, key_rows, value_rows, decay_input, learn_input, decay_base, decay_shift, channel_gain, out_weight)
    expert_out = expert_layer(expert_input, expert_gain, routes, route_weight, gate_weight, up_weight, down_weight)
    return (mixer_out, expert_out)
```

```python
import functools

import jax
import jax.numpy as jnp
from jax import lax
from jax.experimental import pallas as pl
from jax.experimental.pallas import tpu as pltpu
from jax.sharding import PartitionSpec as P

MESH = pl.DeviceIdType.MESH
NORM_EPS = 1e-06
GROUP_EPS = 0.00064
F=jnp.float32; B=jnp.bfloat16
C=64
NT=(((1,),(1,)),((),())); NN=(((1,),(0,)),((),())); TN=(((0,),(0,)),((),()))
def dg(a,b,dims): return lax.dot_general(a,b,dims,preferred_element_type=F)
def split(x):
    hi=x.astype(B); return hi,(x-hi.astype(F)).astype(B)
def dot3(a,b,dims):
    ah,al=split(a); bh,bl=split(b)
    return dg(ah,bh,dims)+(dg(ah,bl,dims)+dg(al,bh,dims))
def fold(x,n): return x[:n]+x[n:]
def consts():
    r=lax.broadcasted_iota(jnp.int32,(128,128),0); c=lax.broadcasted_iota(jnp.int32,(128,128),1)
    same=(r//64)==(c//64)
    return r,c,same
def pre_stage(key,dec,learn,base,s0,s1):
    r,c,same=consts()
    ones=same.astype(B)
    kf=key.astype(F)
    hi,lo=split(kf*kf)
    ss=dg(hi,ones,NN)+dg(lo,ones,NN)
    unit=kf*lax.rsqrt(ss+1e-6)
    lane=lax.broadcasted_iota(jnp.int32,key.shape,1)
    pre=dec.astype(F)+base+jnp.where(lane<64,s0,s1)
    ld=-0.6065306597126334/(1.0+jnp.exp(-pre))
    rem=unit/(1.0+jnp.exp(-learn.astype(F)))
    return kf,unit,ld,rem
def chunk_cum(ld):
    r,c,same=consts()
    tri=(same&(r>=c)).astype(B)
    outs=[]
    for i in range(ld.shape[0]//128):
        hi,lo=split(ld[i*128:(i+1)*128])
        outs.append(dg(tri,hi,NN)+dg(tri,lo,NN))
    return jnp.concatenate(outs,0)
def chunk(rec,kf,vb,unit,rem,ld,cum):
    r,c,same=consts()
    lane=lax.broadcasted_iota(jnp.int32,(C,128),1)
    m0=lane<64
    mid=cum[C//2-1:C//2]; end=cum[C-1:C]
    rel=cum-mid
    Q=rec*jnp.exp(rel); P=unit*jnp.exp(rel-ld)
    sh=jnp.exp(-rel)
    BR=(rem*sh).astype(B); BK=(kf*sh).astype(B)
    Qb=Q.astype(B); Pb=P.astype(B)
    z=jnp.zeros((C,128),B)
    ex=lambda x: jnp.concatenate([jnp.where(m0,x,z),jnp.where(m0,z,x)],0)
    Pe=ex(Pb)
    lhs=jnp.concatenate([Pe,ex(Qb)],0)
    sR=dg(lhs,jnp.concatenate([BR,BR],0),NT)
    sK=dg(lhs,jnp.concatenate([BK,BK],0),NT)
    strict=same&(r>c); incl=same&(r>=c)
    zf=jnp.zeros((128,128),F)
    A=jnp.where(strict,sR[:128],zf).astype(B)
    PK=jnp.where(strict,sK[:128],zf).astype(B)
    QR=jnp.where(incl,sR[128:],zf).astype(B)
    QK=jnp.where(incl,sK[128:],zf).astype(B)
    zb=jnp.zeros((128,128),B)
    x=r^c
    lm=lambda m: (x>=m)&(x<2*m)
    D=jnp.where(r==c,1.0,0.0).astype(B)-jnp.where(lm(1),A,zb)
    m=2
    while m<C:
        E=dg(jnp.where(lm(m),A,zb),D,NN).astype(B)
        D=D-dg(D,E,NN).astype(B)
        m*=2
    Ve=ex(vb)
    kv=dg(jnp.concatenate([PK,QK],0),Ve,NN)
    X=dg(D,jnp.concatenate([Pe,kv[:128].astype(B)],1),NN)
    Xb=X.astype(B)
    qx=dg(QR,Xb,NN)
    em=jnp.exp(mid); et=jnp.exp(end-mid)
    reader=(Q-fold(qx[:,:128],C))*em
    local=fold(kv[128:],C)-fold(qx[:,128:],C)
    X0=fold(Xb[:,:128],C); L=fold(Xb[:,128:],C)
    tx=dg(X0,BR,TN)
    eye=jnp.where(r==c,1.0,0.0).astype(F)
    emT=jnp.sum(jnp.where(r==c,jnp.broadcast_to(em,(128,128)),zf),1,keepdims=True)
    T=jnp.where(same,(eye-tx)*emT*et,zf)
    off=dg(jnp.concatenate([vb,-L],0),jnp.concatenate([BK,BR],0),TN)
    off=jnp.where(same,off*et,zf)
    return reader,local,T,off
def local_scan(rec,key,val,dec,learn,base,s0,s1):
    n=key.shape[0]//C
    kf,unit,ld,rem=pre_stage(key,dec,learn,base,s0,s1)
    cum=chunk_cum(ld)
    outs=[]
    for i in range(n):
        s=slice(i*C,(i+1)*C)
        outs.append(chunk(rec[s].astype(F),kf[s],val[s],unit[s],rem[s],ld[s],cum[s]))
    r,c,same=consts()
    PB=None
    rd=[];lc=[]
    for i in range(n):
        reader,local,T,off=outs[i]
        if PB is None:
            rd.append(reader); lc.append(local)
            PB=jnp.concatenate([T,off],0)
        else:
            ph,pl_=split(PB)
            rh=reader.astype(B)
            q=dg(rh,ph,NT)
            rd.append(q[:,:128]); lc.append(local+q[:,128:])
            PB=dot3(PB,T,NN)+jnp.concatenate([jnp.zeros_like(off),off],0)
    return jnp.concatenate(rd,0),jnp.concatenate(lc,0),PB[:128],PB[128:]


def mix_kernel(rec_ref, key_ref, val_ref, dec_ref, learn_ref, base_ref, shift_ref, rd_ref, lc_ref, mb_ref):
    pair = pl.program_id(0)
    shift = shift_ref[...]
    heads = lax.broadcasted_iota(jnp.int32, shift.shape, 1)
    s0 = jnp.sum(jnp.where(heads == 2 * pair, shift, 0.0), 1, keepdims=True)
    s1 = jnp.sum(jnp.where(heads == 2 * pair + 1, shift, 0.0), 1, keepdims=True)
    rd, lc, whole, offset = local_scan(
        rec_ref[...], key_ref[...], val_ref[...], dec_ref[...], learn_ref[...], base_ref[...], s0, s1
    )
    rd_ref[...] = rd.astype(B)
    lc_ref[...] = lc
    r, c, same = consts()
    less = fold(whole - jnp.where(r == c, 1.0, 0.0), C)
    mb_ref[0] = jnp.concatenate([less, fold(offset, C)], 0).astype(B)


def mix_local(rec, key, val, dec, learn, base, shift):
    rows, channels = rec.shape
    pairs = channels // 128
    slab = pl.BlockSpec((rows, 128), lambda p: (0, p))
    return pl.pallas_call(
        mix_kernel,
        grid=(pairs,),
        in_specs=[slab] * 5
        + [pl.BlockSpec((1, 128), lambda p: (0, p)), pl.BlockSpec(shift.shape, lambda p: (0, 0))],
        out_specs=[slab, slab, pl.BlockSpec((1, 128, 128), lambda p: (p, 0, 0))],
        out_shape=[
            jax.ShapeDtypeStruct((rows, channels), B),
            jax.ShapeDtypeStruct((rows, channels), F),
            jax.ShapeDtypeStruct((pairs, 128, 128), B),
        ],
        cost_estimate=pl.CostEstimate(flops=12_000_000_000, bytes_accessed=5_000_000, transcendentals=1_000_000),
        name="mix_local",
    )(rec, key, val, dec, learn, base.reshape(1, channels), shift)


def spread(compact):
    lane = lax.broadcasted_iota(jnp.int32, compact.shape, 1)
    nil = jnp.zeros_like(compact)
    return jnp.concatenate([jnp.where(lane < 64, compact, nil), jnp.where(lane < 64, nil, compact)], 0)


def unpack(message):
    r, c, same = consts()
    eye = jnp.where(r == c, 1.0, 0.0).astype(F)
    wide = message.astype(F)
    return spread(wide[:C]) + eye, wide[C:]


def prefix_kernel(mb_ref, out_ref, row_buf, exc_buf, tz_buf, z_buf, fin_buf, s1, r1, s2, r2, s3, r3):
    ep = lax.axis_index("ep")
    z, m = ep // 8, ep % 8
    x, core = m // 2, m % 2
    barrier = pltpu.get_barrier_semaphore()
    for d in range(1, 8):
        pl.semaphore_signal(barrier, inc=1, device_id={"ep": z * 8 + (m + d) % 8}, device_id_type=MESH)
        pl.semaphore_signal(barrier, inc=1, device_id={"ep": ((z + d) % 8) * 8 + m}, device_id_type=MESH)
    pl.semaphore_wait(barrier, 14)

    def to_row(d):
        j = (m + d) % 8
        return pltpu.make_async_remote_copy(
            src_ref=mb_ref.at[j // 2], dst_ref=row_buf.at[m], send_sem=s1.at[d], recv_sem=r1.at[m],
            device_id={"ep": z * 8 + j}, device_id_type=MESH,
        )

    def from_row(d):
        j = (m + d) % 8
        return pltpu.make_async_remote_copy(
            src_ref=mb_ref.at[0], dst_ref=row_buf.at[j], send_sem=s1.at[d], recv_sem=r1.at[j],
            device_id={"ep": z * 8 + j}, device_id_type=MESH,
        )

    for d in range(1, 8):
        to_row(d).start()
    row_buf[m] = mb_ref[x]
    for d in range(1, 8):
        from_row(d).wait_recv()

    r, c, same = consts()
    eye = jnp.where(r == c, 1.0, 0.0).astype(F)
    running = jnp.concatenate([fold(eye, C), jnp.zeros((C, 128), F)], 0)
    for j in range(8):
        exc_buf[j] = running
        step, offset = unpack(row_buf[j])
        if j == 0:
            running = jnp.concatenate([fold(step, C), offset], 0)
        else:
            running = dot3(running, step, NN) + jnp.concatenate([jnp.zeros((C, 128), F), offset], 0)
    tz_buf[...] = (running - jnp.concatenate([fold(eye, C), jnp.zeros((C, 128), F)], 0)).astype(B)

    def to_z(d):
        there = (z + d) % 8
        return pltpu.make_async_remote_copy(
            src_ref=tz_buf, dst_ref=z_buf.at[z], send_sem=s2.at[d], recv_sem=r2.at[z],
            device_id={"ep": there * 8 + m}, device_id_type=MESH,
        )

    def from_z(d):
        there = (z + d) % 8
        return pltpu.make_async_remote_copy(
            src_ref=tz_buf, dst_ref=z_buf.at[there], send_sem=s2.at[d], recv_sem=r2.at[there],
            device_id={"ep": there * 8 + m}, device_id_type=MESH,
        )

    for d in range(1, 8):
        to_z(d).start()
    z_buf[z] = tz_buf[...]
    for d in range(1, 8):
        from_z(d).wait_recv()
    state = jnp.zeros((C, 128), F)
    for j in range(7):
        step, offset = unpack(z_buf[j])
        after = offset if j == 0 else dot3(state, step, NN) + offset
        state = jnp.where(j < z, after, state)
    for k in range(4):
        member = exc_buf[k * 2 + core]
        fin_buf[k] = (dot3(state, spread(member[:C]), NN) + member[C:]).astype(B)

    def to_member(d):
        k = (x + d) % 4
        return pltpu.make_async_remote_copy(
            src_ref=fin_buf.at[k], dst_ref=out_ref.at[x], send_sem=s3.at[d], recv_sem=r3.at[x],
            device_id={"ep": z * 8 + k * 2 + core}, device_id_type=MESH,
        )

    def from_member(d):
        k = (x + d) % 4
        return pltpu.make_async_remote_copy(
            src_ref=fin_buf.at[k], dst_ref=out_ref.at[k], send_sem=s3.at[d], recv_sem=r3.at[k],
            device_id={"ep": z * 8 + k * 2 + core}, device_id_type=MESH,
        )

    for d in range(1, 4):
        to_member(d).start()
    out_ref[x] = fin_buf[x]
    for d in range(1, 4):
        from_member(d).wait_recv()
    for d in range(1, 8):
        to_row(d).wait_send()
        to_z(d).wait_send()
    for d in range(1, 4):
        to_member(d).wait_send()


def prefix(mb):
    vmem = pl.BlockSpec(memory_space=pltpu.VMEM)
    dma = pltpu.SemaphoreType.DMA
    return pl.pallas_call(
        prefix_kernel,
        in_specs=[vmem],
        out_specs=vmem,
        out_shape=jax.ShapeDtypeStruct((4, C, 128), B),
        scratch_shapes=[
            pltpu.VMEM((8, 128, 128), B),
            pltpu.VMEM((8, 128, 128), F),
            pltpu.VMEM((128, 128), B),
            pltpu.VMEM((8, 128, 128), B),
            pltpu.VMEM((4, C, 128), B),
            dma((8,)), dma((8,)), dma((8,)), dma((8,)), dma((4,)), dma((4,)),
        ],
        compiler_params=pltpu.CompilerParams(collective_id=0, has_side_effects=True),
        cost_estimate=pl.CostEstimate(flops=4_000_000_000, bytes_accessed=1_000_000, transcendentals=0),
        name="prefix",
    )(mb)


def head_sum(x, ones):
    hi, lo = split(x)
    return dg(hi, ones, NN) + dg(lo, ones, NN)


def project_kernel(rd_ref, lc_ref, state_ref, gain_ref, w_ref, out_ref):
    r, c, same = consts()
    ones = jnp.where(same, 1.0 / 64, 0.0).astype(B)
    parts = []
    for p in range(rd_ref.shape[1] // 128):
        lanes = slice(p * 128, (p + 1) * 128)
        read = lc_ref[:, lanes] + dg(rd_ref[:, lanes], spread(state_ref[p]), NT)
        centred = read - head_sum(read, ones)
        variance = head_sum(centred * centred, ones)
        parts.append((centred * lax.rsqrt(variance + GROUP_EPS) * gain_ref[:, lanes]).astype(B))
    out_ref[...] = dg(jnp.concatenate(parts, 1), w_ref[...], NN).astype(B)


def project(rd, lc, state, gain, w_out):
    rows, channels = rd.shape
    width = w_out.shape[1]
    block = 128
    return pl.pallas_call(
        project_kernel,
        grid=(rows // block,),
        in_specs=[
            pl.BlockSpec((block, channels), lambda i: (i, 0)),
            pl.BlockSpec((block, channels), lambda i: (i, 0)),
            pl.BlockSpec(state.shape, lambda i: (0, 0, 0)),
            pl.BlockSpec((1, channels), lambda i: (0, 0)),
            pl.BlockSpec(w_out.shape, lambda i: (0, 0)),
        ],
        out_specs=pl.BlockSpec((block, width), lambda i: (i, 0)),
        out_shape=jax.ShapeDtypeStruct((rows, width), B),
        cost_estimate=pl.CostEstimate(flops=2_000_000_000, bytes_accessed=6_000_000, transcendentals=0),
        name="project",
    )(rd, lc, state, gain.reshape(1, channels), w_out)


def expert_kernel(x_ref, *refs):
    weights, (out_ref, *scratch) = refs[:13], refs[13:]
    g_buf, u_buf, d_buf, acc, sems = scratch
    half = d_buf.shape[1] // 2
    targets = []
    for s in range(4):
        targets += [g_buf.at[s], u_buf.at[s]]
        if s < 3:
            targets.append(d_buf.at[s])
        else:
            targets += [d_buf.at[s, pl.ds(0, half)], d_buf.at[s, pl.ds(half, half)]]
    copies = [pltpu.make_async_copy(w, t, sems.at[i]) for i, (w, t) in enumerate(zip(weights, targets))]
    for copy in copies:
        copy.start()
    rows = 128
    for s in range(4):
        for copy in copies[3 * s : 3 * s + (3 if s < 3 else 4)]:
            copy.wait()

        @pl.loop(0, x_ref.shape[0] // rows)
        def _(i):
            here = pl.ds(pl.multiple_of(i * rows, rows), rows)
            x = x_ref[here, :]
            gate = dg(x, g_buf[s], NN)
            up = dg(x, u_buf[s], NN)
            hidden = (gate / (1.0 + jnp.exp(-gate)) * up).astype(B)
            part = dg(hidden, d_buf[s], NN)
            if s == 0:
                acc[here, :] = part
            elif s < 3:
                acc[here, :] += part
            else:
                out_ref[here, :] = (acc[here, :] + part).astype(B)


def expert(x, shards):
    vmem = pl.BlockSpec(memory_space=pltpu.VMEM)
    rows, width = x.shape
    flat = [w for shard in shards for w in shard]
    depth, units = shards[0][0].shape
    return pl.pallas_call(
        expert_kernel,
        in_specs=[vmem] + [pl.BlockSpec(memory_space=pl.ANY)] * len(flat),
        out_specs=vmem,
        out_shape=jax.ShapeDtypeStruct((rows, width), B),
        scratch_shapes=[
            pltpu.VMEM((4, depth, units), B),
            pltpu.VMEM((4, depth, units), B),
            pltpu.VMEM((4, units, width), B),
            pltpu.VMEM((rows, width), F),
            pltpu.SemaphoreType.DMA((len(flat),)),
        ],
        compiler_params=pltpu.CompilerParams(vmem_limit_bytes=48 * 1024 * 1024),
        cost_estimate=pl.CostEstimate(flops=13_000_000_000, bytes_accessed=17_000_000, transcendentals=500_000),
        name="expert",
    )(x, *flat)


def slot_targets(block_routes, experts, capacity):
    flat_routes = block_routes.reshape(-1)
    matches = (flat_routes[:, None] == jnp.arange(experts, dtype=jnp.int32)[None, :]).astype(jnp.int32)
    earlier = jnp.cumsum(matches, axis=0) - matches
    slots = jnp.sum(earlier * matches, axis=1).reshape(block_routes.shape)
    return block_routes * capacity + slots


def on_device(
    receptance, key_rows, value_rows, decay_input, learn_input, decay_base, decay_shift, channel_gain,
    out_weight, expert_input, expert_gain, routes, route_weight, gate_weight, up_weight, down_weight,
):
    ep_count = lax.axis_size("ep")
    token_rows, width = expert_input.shape
    top_count = routes.shape[1]
    experts = gate_weight.shape[0] * ep_count
    capacity = max(2, 2 * token_rows * top_count // experts)
    ahead = [(i, (i + 1) % 4) for i in range(4)]
    back = [(i, (i + 3) % 4) for i in range(4)]
    own = [gate_weight[0], up_weight[0], down_weight[0]]
    near = [[lax.ppermute(w, "tp", ring) for w in own] for ring in (ahead, back)]
    half = own[2].shape[0] // 2
    far = [
        lax.ppermute(near[0][0], "tp", ahead),
        lax.ppermute(near[1][1], "tp", back),
        lax.ppermute(near[0][2][:half], "tp", ahead),
        lax.ppermute(near[1][2][half:], "tp", back),
    ]

    inputs = expert_input.astype(F)
    normed = (
        inputs * lax.rsqrt(jnp.mean(inputs * inputs, axis=1, keepdims=True) + NORM_EPS) * expert_gain
    ).astype(B)
    targets = slot_targets(routes, experts, capacity)
    places = jnp.arange(experts * capacity, dtype=jnp.int32)
    marks = (places[:, None, None] == targets[None, :, :]).astype(jnp.int32)
    outgoing = jnp.dot(jnp.sum(marks, axis=2).astype(B), normed, preferred_element_type=F).astype(B)
    arrived = lax.all_to_all(
        outgoing.reshape(experts, capacity, width), "ep", split_axis=0, concat_axis=0, tiled=True
    )

    rd, lc, mb = mix_local(
        receptance, key_rows, value_rows, decay_input, learn_input, decay_base, decay_shift
    )
    state = prefix(mb)
    part = project(rd, lc, state, channel_gain, out_weight)
    pieces = lax.all_to_all(part.reshape(4, -1, width), "tp", 0, 0, tiled=True)
    mixer_out = jnp.sum(pieces.astype(F), axis=0).astype(B)

    rows = expert(arrived.reshape(ep_count * capacity, width), [own, near[0], near[1], far])
    returned = lax.all_to_all(
        rows.reshape(ep_count, capacity, width), "ep", split_axis=0, concat_axis=0, tiled=True
    ).reshape(experts * capacity, width)
    weights = jnp.sum(
        jnp.where(places[None, :, None] == targets[:, None, :], route_weight[:, None, :], 0.0), axis=2
    )
    hi, lo = split(weights)
    combined = dg(hi, returned, NN) + dg(lo, returned, NN)
    return (mixer_out, combined.astype(B))


def solution(mesh):
    both = P(("ep", "tp"), None)
    placed = (
        P("ep", "tp"), P("ep", "tp"), P("ep", "tp"), P("ep", "tp"), P("ep", "tp"), P("tp"), P("ep", "tp"), P("tp"),
        P("tp", None), both, P(), both, both, P("ep", None, "tp"), P("ep", None, "tp"), P("ep", "tp", None),
    )
    return jax.shard_map(on_device, mesh=mesh, in_specs=placed, out_specs=(both, both), check_vma=False)
```

```python
import functools

import jax
import jax.numpy as jnp
from jax import lax
from jax.experimental import pallas as pl
from jax.experimental.pallas import tpu as pltpu
from jax.sharding import PartitionSpec as P


MESH = pl.DeviceIdType.MESH
NORM_EPS = 1e-06
GROUP_EPS = 0.00064
F=jnp.float32; B=jnp.bfloat16
C=64
NT=(((1,),(1,)),((),())); NN=(((1,),(0,)),((),())); TN=(((0,),(0,)),((),()))
def dg(a,b,dims): return lax.dot_general(a,b,dims,preferred_element_type=F)
def split(x):
    hi=x.astype(B); return hi,(x-hi.astype(F)).astype(B)
def dot3(a,b,dims):
    ah,al=split(a); bh,bl=split(b)
    return dg(ah,bh,dims)+(dg(ah,bl,dims)+dg(al,bh,dims))
def fold(x,n): return x[:n]+x[n:]
def consts():
    r=lax.broadcasted_iota(jnp.int32,(128,128),0); c=lax.broadcasted_iota(jnp.int32,(128,128),1)
    same=(r//64)==(c//64)
    return r,c,same
def pre_stage(key,dec,learn,base,s0,s1):
    r,c,same=consts()
    ones=same.astype(B)
    kf=key.astype(F)
    hi,lo=split(kf*kf)
    ss=dg(hi,ones,NN)+dg(lo,ones,NN)
    unit=kf*lax.rsqrt(ss+1e-6)
    lane=lax.broadcasted_iota(jnp.int32,key.shape,1)
    pre=dec.astype(F)+base+jnp.where(lane<64,s0,s1)
    ld=-0.6065306597126334/(1.0+jnp.exp(-pre))
    rem=unit/(1.0+jnp.exp(-learn.astype(F)))
    return kf,unit,ld,rem
def chunk_cum(ld):
    r,c,same=consts()
    tri=(same&(r>=c)).astype(B)
    outs=[]
    for i in range(ld.shape[0]//128):
        hi,lo=split(ld[i*128:(i+1)*128])
        outs.append(dg(tri,hi,NN)+dg(tri,lo,NN))
    return jnp.concatenate(outs,0)
def chunk(rec,kf,vb,unit,rem,ld,cum):
    r,c,same=consts()
    lane=lax.broadcasted_iota(jnp.int32,(C,128),1)
    m0=lane<64
    mid=cum[C//2-1:C//2]; end=cum[C-1:C]
    rel=cum-mid
    Q=rec*jnp.exp(rel); P=unit*jnp.exp(rel-ld)
    sh=jnp.exp(-rel)
    BR=(rem*sh).astype(B); BK=(kf*sh).astype(B)
    Qb=Q.astype(B); Pb=P.astype(B)
    z=jnp.zeros((C,128),B)
    ex=lambda x: jnp.concatenate([jnp.where(m0,x,z),jnp.where(m0,z,x)],0)
    Pe=ex(Pb)
    lhs=jnp.concatenate([Pe,ex(Qb)],0)
    sR=dg(lhs,jnp.concatenate([BR,BR],0),NT)
    sK=dg(lhs,jnp.concatenate([BK,BK],0),NT)
    yield None
    strict=same&(r>c); incl=same&(r>=c)
    zf=jnp.zeros((128,128),F)
    A=jnp.where(strict,sR[:128],zf).astype(B)
    PK=jnp.where(strict,sK[:128],zf).astype(B)
    QR=jnp.where(incl,sR[128:],zf).astype(B)
    QK=jnp.where(incl,sK[128:],zf).astype(B)
    zb=jnp.zeros((128,128),B)
    x=r^c
    lm=lambda m: (x>=m)&(x<2*m)
    D=jnp.where(r==c,1.0,0.0).astype(B)-jnp.where(lm(1),A,zb)
    m=2
    while m<C:
        E=dg(jnp.where(lm(m),A,zb),D,NN).astype(B)
        yield None
        D=D-dg(D,E,NN).astype(B)
        yield None
        m*=2
    Ve=ex(vb)
    kv=dg(jnp.concatenate([PK,QK],0),Ve,NN)
    yield None
    X=dg(D,jnp.concatenate([Pe,kv[:128].astype(B)],1),NN)
    Xb=X.astype(B)
    yield None
    qx=dg(QR,Xb,NN)
    yield None
    em=jnp.exp(mid); et=jnp.exp(end-mid)
    reader=(Q-fold(qx[:,:128],C))*em
    local=fold(kv[128:],C)-fold(qx[:,128:],C)
    X0=fold(Xb[:,:128],C); L=fold(Xb[:,128:],C)
    tx=dg(X0,BR,TN)
    yield None
    eye=jnp.where(r==c,1.0,0.0).astype(F)
    emT=jnp.sum(jnp.where(r==c,jnp.broadcast_to(em,(128,128)),zf),1,keepdims=True)
    T=jnp.where(same,(eye-tx)*emT*et,zf)
    off=dg(jnp.concatenate([vb,-L],0),jnp.concatenate([BK,BR],0),TN)
    off=jnp.where(same,off*et,zf)
    yield reader,local,T,off
def local_scan(rec,key,val,dec,learn,base,s0,s1):
    n=key.shape[0]//C
    kf,unit,ld,rem=pre_stage(key,dec,learn,base,s0,s1)
    cum=chunk_cum(ld)
    outs=[]
    for i in range(n):
        s=slice(i*C,(i+1)*C)
        outs.append(chunk(rec[s].astype(F),kf[s],val[s],unit[s],rem[s],ld[s],cum[s]))
    while True:
        now=[next(o) for o in outs]
        if now[0] is not None: break
    outs=now
    r,c,same=consts()
    PB=None
    rd=[];lc=[]
    for i in range(n):
        reader,local,T,off=outs[i]
        if PB is None:
            rd.append(reader); lc.append(local)
            PB=jnp.concatenate([T,off],0)
        else:
            ph,pl_=split(PB)
            rh=reader.astype(B)
            q=dg(rh,ph,NT)
            rd.append(q[:,:128]); lc.append(local+q[:,128:])
            PB=dot3(PB,T,NN)+jnp.concatenate([jnp.zeros_like(off),off],0)
    return jnp.concatenate(rd,0),jnp.concatenate(lc,0),PB[:128],PB[128:]


def spread(compact):
    lane = lax.broadcasted_iota(jnp.int32, compact.shape, 1)
    nil = jnp.zeros_like(compact)
    return jnp.concatenate([jnp.where(lane < 64, compact, nil), jnp.where(lane < 64, nil, compact)], 0)


def unpack(message):
    r, c, same = consts()
    eye = jnp.where(r == c, 1.0, 0.0).astype(F)
    wide = message.astype(F)
    return spread(wide[:C]) + eye, wide[C:]


def head_sum(x, ones):
    hi, lo = split(x)
    return dg(hi, ones, NN) + dg(lo, ones, NN)


def remote(src, dst, send, recv, where):
    return pltpu.make_async_remote_copy(
        src_ref=src, dst_ref=dst, send_sem=send, recv_sem=recv, device_id=where, device_id_type=MESH
    )


def wait_bytes(ref, sem):
    pltpu.make_async_copy(ref, ref, sem).wait()


def kernel(
    rec_hbm, key_hbm, val_hbm, dec_hbm, learn_hbm, wout_hbm, x_hbm, gate_hbm, up_hbm, down_hbm,
    base_ref, shift_ref, gain_ref, xgain_ref, routes_ref, rw_ref,
    mixer_ref, expert_ref,
    mix_in, wout, xin, g_buf, u_buf, d_buf, rd_buf, lc_buf, mb_buf, row_buf, exc_buf, tz_buf, z_buf, fin_buf, st_buf,
    wt_buf, out_buf, arr_buf, acc, res_buf, ret_buf, part_buf, rs_buf,
    in_sems, own_sems, ws, wr, s1, r1, s2, r2, s3, r3, s4, r4, misc, go,
):
    ep, tp = lax.axis_index("ep"), lax.axis_index("tp")
    z, m = ep // 8, ep % 8
    x, core = m // 2, m % 2
    n = 64
    right, left = (tp + 1) % 4, (tp + 3) % 4

    loads = [pltpu.make_async_copy(x_hbm, xin, in_sems.at[0])]
    for i, src in enumerate((rec_hbm, key_hbm, val_hbm, dec_hbm, learn_hbm)):
        loads.append(pltpu.make_async_copy(src, mix_in.at[i], in_sems.at[i + 1]))
    loads.append(pltpu.make_async_copy(wout_hbm, wout, in_sems.at[6]))
    own = [
        pltpu.make_async_copy(src, dst.at[0], own_sems.at[i])
        for i, (src, dst) in enumerate(((gate_hbm, g_buf), (up_hbm, u_buf), (down_hbm, d_buf)))
    ]
    for load in loads + own:
        load.start()

    barrier = pltpu.get_barrier_semaphore()

    @pl.loop(1, n)
    def _(d):
        pl.semaphore_signal(barrier, inc=1, device_id={"ep": (ep + d) % n}, device_id_type=MESH)

    for d in range(1, 4):
        pl.semaphore_signal(barrier, inc=1, device_id={"tp": (tp + d) % 4}, device_id_type=MESH)
    pl.semaphore_wait(barrier, n - 1 + 3)

    half = d_buf.shape[1] // 2
    top, bottom = pl.ds(0, half), pl.ds(half, half)
    ahead, back = {"tp": right}, {"tp": left}
    near = [
        remote(gate_hbm, g_buf.at[1], ws.at[0], wr.at[0], ahead),
        remote(up_hbm, u_buf.at[2], ws.at[1], wr.at[1], back),
        remote(down_hbm, d_buf.at[1], ws.at[2], wr.at[2], ahead),
        remote(down_hbm, d_buf.at[2], ws.at[3], wr.at[3], back),
        remote(up_hbm, u_buf.at[1], ws.at[4], wr.at[4], ahead),
        remote(gate_hbm, g_buf.at[2], ws.at[5], wr.at[5], back),
    ]
    far = [
        remote(g_buf.at[1], g_buf.at[3], ws.at[6], wr.at[6], ahead),
        remote(u_buf.at[2], u_buf.at[3], ws.at[7], wr.at[7], back),
        remote(d_buf.at[1, top], d_buf.at[3, top], ws.at[8], wr.at[8], ahead),
        remote(d_buf.at[2, bottom], d_buf.at[3, bottom], ws.at[9], wr.at[9], back),
    ]

    def forward():
        for i in range(4):
            near[i].wait_recv()
            far[i].start()

    @pl.when(core == 0)
    def _():
        for copy in near:
            copy.start()

    loads[0].wait()
    rows = xin[...].astype(F)
    normed = (rows * lax.rsqrt(jnp.mean(rows * rows, axis=1, keepdims=True) + NORM_EPS) * xgain_ref[...]).astype(B)
    named = routes_ref[...]
    r0, r1_ = named[:, 0:1], named[:, 1:2]
    r, c, same = consts()
    hits = ((c == r0) | (c == r1_)).astype(F).astype(B)
    earlier = dg((r > c).astype(F).astype(B), hits, NN)
    t0 = r0.astype(F) * 8.0 + jnp.sum(jnp.where(c == r0, earlier, 0.0), 1, keepdims=True)
    t1 = r1_.astype(F) * 8.0 + jnp.sum(jnp.where(c == r1_, earlier, 0.0), 1, keepdims=True)
    place = lax.broadcasted_iota(jnp.int32, (128, n * 8), 1).astype(F)
    first, second = place == t0, place == t1
    marks = jnp.where(first | second, 1.0, 0.0).astype(B)
    shares = jnp.where(first, rw_ref[:, 0:1], 0.0) + jnp.where(second, rw_ref[:, 1:2], 0.0)
    hi, lo = split(shares)
    wt_buf[0] = hi
    wt_buf[1] = lo
    for b in range(4):
        out_buf[16 * b : 16 * b + 16] = (
            dg(marks[:, 128 * b : 128 * b + 128], normed, TN).reshape(16, 8, -1).astype(B)
        )

    def send_rows(src, dst, sem, there):
        remote(src.at[there], dst.at[ep], sem.at[0], sem.at[1], {"ep": there}).start()

    @pl.loop(0, n // 2)
    def _(d):
        send_rows(out_buf, arr_buf, s4, (ep + 2 * d + 1) % n)

    for load in loads[1:6]:
        load.wait()

    @pl.loop(0, 4)
    def _(p):
        lanes = pl.ds(pl.multiple_of(p * 128, 128), 128)
        shift = shift_ref[...]
        heads = lax.broadcasted_iota(jnp.int32, shift.shape, 1)
        h0 = jnp.sum(jnp.where(heads == 2 * p, shift, 0.0), 1, keepdims=True)
        h1 = jnp.sum(jnp.where(heads == 2 * p + 1, shift, 0.0), 1, keepdims=True)
        a = [mix_in[i, :, lanes] for i in range(5)]
        rd, lc, whole, offset = local_scan(*a, base_ref[:, lanes], h0, h1)
        rd_buf[:, lanes] = rd.astype(B)
        lc_buf[:, lanes] = lc
        r, c, same = consts()
        less = fold(whole - jnp.where(r == c, 1.0, 0.0), C)
        mb_buf[p] = jnp.concatenate([less, fold(offset, C)], 0).astype(B)

    def row_copy(d, slot):
        j = (m + d) % 8
        return remote(mb_buf.at[j // 2], row_buf.at[slot], s1.at[d], r1.at[slot], {"ep": z * 8 + j})

    for d in range(1, 8):
        row_copy(d, m).start()

    @pl.when(core == 0)
    def _():
        forward()

    row_buf[m] = mb_buf[x]
    for d in range(1, 8):
        row_copy(d, (m + d) % 8).wait_recv()
    eye = fold(jnp.where(r == c, 1.0, 0.0).astype(F), C)
    none = jnp.zeros((C, 128), F)
    running = jnp.concatenate([eye, none], 0)
    for j in range(8):
        exc_buf[j] = running
        step, offset = unpack(row_buf[j])
        if j == 0:
            running = jnp.concatenate([fold(step, C), offset], 0)
        else:
            running = dot3(running, step, NN) + jnp.concatenate([none, offset], 0)
    tz_buf[...] = (running - jnp.concatenate([eye, none], 0)).astype(B)

    def z_copy(d, slot):
        return remote(tz_buf, z_buf.at[slot], s2.at[d], r2.at[slot], {"ep": ((z + d) % 8) * 8 + m})

    for d in range(1, 8):
        z_copy(d, z).start()

    @pl.loop(1, n // 2)
    def _(d):
        send_rows(out_buf, arr_buf, s4, (ep + 2 * d) % n)

    arr_buf[ep] = out_buf[ep]
    z_buf[z] = tz_buf[...]
    for d in range(1, 8):
        z_copy(d, (z + d) % 8).wait_recv()
    state = none
    for j in range(7):
        step, offset = unpack(z_buf[j])
        after = offset if j == 0 else dot3(state, step, NN) + offset
        state = jnp.where(j < z, after, state)
    for k in range(4):
        member = exc_buf[k * 2 + core]
        fin_buf[k] = (dot3(state, spread(member[:C]), NN) + member[C:]).astype(B)

    def fin_copy(d, slot):
        k = (x + d) % 4
        return remote(fin_buf.at[k], st_buf.at[slot], s3.at[d], r3.at[slot], {"ep": z * 8 + k * 2 + core})

    for d in range(1, 4):
        fin_copy(d, x).start()

    @pl.when(core == 1)
    def _():
        for copy in near:
            copy.start()

    st_buf[x] = fin_buf[x]
    for d in range(1, 4):
        fin_copy(d, (x + d) % 4).wait_recv()

    loads[6].wait()
    ones = jnp.where(same, 1.0 / 64, 0.0).astype(B)
    for b in range(4):
        here = slice(128 * b, 128 * b + 128)
        parts = []
        for p in range(4):
            lanes = slice(p * 128, (p + 1) * 128)
            read = lc_buf[here, lanes] + dg(rd_buf[here, lanes], spread(st_buf[p]), NT)
            centred = read - head_sum(read, ones)
            variance = head_sum(centred * centred, ones)
            parts.append((centred * lax.rsqrt(variance + GROUP_EPS) * gain_ref[:, lanes]).astype(B))
        part_buf[b] = dg(jnp.concatenate(parts, 1), wout[...], NN).astype(B)

    wait_bytes(arr_buf.at[pl.ds(0, n - 1)], s4.at[1])
    for copy in own:
        copy.wait()

    def units(s, b):
        given = arr_buf[pl.ds(16 * b, 16)].reshape(128, -1)
        gate = dg(given, g_buf[s], NN)
        up = dg(given, u_buf[s], NN)
        hidden = (gate / (1.0 + jnp.exp(-gate)) * up).astype(B)
        return dg(hidden, d_buf[s], NN)

    def rows_of(b):
        return pl.ds(pl.multiple_of(b * 128, 128), 128)

    @pl.loop(0, 4)
    def _(b):
        acc[rows_of(b), :] = units(0, b)

    @pl.when(core == 1)
    def _():
        forward()

    near[4].wait_recv()

    @pl.loop(0, 4)
    def _(b):
        acc[rows_of(b), :] += units(1, b)

    near[5].wait_recv()

    @pl.loop(0, 4)
    def _(b):
        acc[rows_of(b), :] += units(2, b)

    for copy in far:
        copy.wait_recv()

    @pl.when(core == 1)
    def _():
        pl.semaphore_signal(go, inc=1, device_id={"ep": ep - 1}, device_id_type=MESH)

    @pl.loop(0, 4)
    def _(i):
        b = (z // 2 + i) % 4
        res_buf[pl.ds(16 * b, 16)] = (acc[rows_of(b), :] + units(3, b)).reshape(16, 8, -1).astype(B)

        @pl.loop(0, 16)
        def _(k):
            there = 16 * b + (ep + k) % 16

            @pl.when(there != ep)
            def _():
                send_rows(res_buf, ret_buf, misc, there)

    @pl.when(core == 0)
    def _():
        pl.semaphore_wait(go, 1)

    def rs_copy(d, slot):
        j = (tp + d) % 4
        return remote(part_buf.at[j], rs_buf.at[slot], ws.at[9 + d], wr.at[10 + slot], {"tp": j})

    for d in range(1, 4):
        rs_copy(d, tp).start()
    ret_buf[ep] = res_buf[ep]
    total = part_buf[tp].astype(F)
    for d in range(1, 4):
        rs_copy(d, (tp + d) % 4).wait_recv()
        total += rs_buf[(tp + d) % 4].astype(F)
    mixer_ref[...] = total.astype(B)

    wait_bytes(ret_buf.at[pl.ds(0, n - 1)], misc.at[1])
    back_rows = ret_buf[...].reshape(n * 8, -1)
    expert_ref[...] = (dg(wt_buf[0], back_rows, NN) + dg(wt_buf[1], back_rows, NN)).astype(B)

    for copy in near + far:
        copy.wait_send()
    for d in range(1, 8):
        row_copy(d, m).wait_send()
        z_copy(d, z).wait_send()
    for d in range(1, 4):
        fin_copy(d, x).wait_send()
        rs_copy(d, tp).wait_send()
    wait_bytes(out_buf.at[pl.ds(0, n - 1)], s4.at[0])
    wait_bytes(res_buf.at[pl.ds(0, n - 1)], misc.at[0])


def on_device(
    receptance, key_rows, value_rows, decay_input, learn_input, decay_base, decay_shift, channel_gain,
    out_weight, expert_input, expert_gain, routes, route_weight, gate_weight, up_weight, down_weight,
):
    t, width = expert_input.shape
    rows, channels = receptance.shape
    depth, units = gate_weight.shape[1:]
    vmem = pl.BlockSpec(memory_space=pltpu.VMEM)
    anywhere = pl.BlockSpec(memory_space=pl.ANY)
    dma = pltpu.SemaphoreType.DMA
    V = pltpu.VMEM
    return pl.pallas_call(
        kernel,
        in_specs=[anywhere] * 10 + [vmem] * 6,
        out_specs=[vmem, vmem],
        out_shape=[jax.ShapeDtypeStruct((t, width), B)] * 2,
        scratch_shapes=[
            V((5, rows, channels), B), V((channels, width), B), V((t, width), B),
            V((4, depth, units), B), V((4, depth, units), B), V((4, units, width), B),
            V((rows, channels), B), V((rows, channels), F),
            V((4, 128, 128), B), V((8, 128, 128), B), V((8, 128, 128), F), V((128, 128), B), V((8, 128, 128), B),
            V((4, C, 128), B), V((4, C, 128), B),
            V((2, t, 512), B), V((64, 8, width), B), V((64, 8, width), B), V((512, width), F),
            V((64, 8, width), B), V((64, 8, width), B), V((4, t, width), B), V((4, t, width), B),
            dma((7,)), dma((3,)), dma((13,)), dma((14,)), dma((8,)), dma((8,)), dma((8,)), dma((8,)), dma((4,)), dma((4,)),
            dma((2,)), dma((2,)), dma((2,)), pltpu.SemaphoreType.REGULAR,
        ],
        compiler_params=pltpu.CompilerParams(
            collective_id=0, has_side_effects=True, vmem_limit_bytes=60 * 1024 * 1024
        ),
        name="step",
    )(
        receptance, key_rows, value_rows, decay_input, learn_input, out_weight, expert_input,
        gate_weight[0], up_weight[0], down_weight[0],
        decay_base.reshape(1, channels), decay_shift, channel_gain.reshape(1, channels), expert_gain.reshape(1, width),
        routes, route_weight,
    )


def solution(mesh):
    both = P(("ep", "tp"), None)
    placed = (
        P("ep", "tp"), P("ep", "tp"), P("ep", "tp"), P("ep", "tp"), P("ep", "tp"), P("tp"), P("ep", "tp"), P("tp"),
        P("tp", None), both, P(), both, both, P("ep", None, "tp"), P("ep", None, "tp"), P("ep", "tp", None),
    )
    return jax.shard_map(on_device, mesh=mesh, in_specs=placed, out_specs=(both, both), check_vma=False)
```

```python
import functools

import jax
import jax.numpy as jnp
from jax import lax
from jax.experimental import pallas as pl
from jax.experimental.pallas import tpu as pltpu
from jax.sharding import PartitionSpec as P


MESH = pl.DeviceIdType.MESH
NORM_EPS = 1e-06
GROUP_EPS = 0.00064
F=jnp.float32; B=jnp.bfloat16
C=64
NT=(((1,),(1,)),((),())); NN=(((1,),(0,)),((),())); TN=(((0,),(0,)),((),()))
def dg(a,b,dims): return lax.dot_general(a,b,dims,preferred_element_type=F)
def split(x):
    hi=x.astype(B); return hi,(x-hi.astype(F)).astype(B)
def dot3(a,b,dims):
    ah,al=split(a); bh,bl=split(b)
    return dg(ah,bh,dims)+(dg(ah,bl,dims)+dg(al,bh,dims))
def fold(x,n): return x[:n]+x[n:]
def consts():
    r=lax.broadcasted_iota(jnp.int32,(128,128),0); c=lax.broadcasted_iota(jnp.int32,(128,128),1)
    same=(r//64)==(c//64)
    return r,c,same
def pre_stage(key,dec,learn,base,shift):
    r,c,same=consts()
    ones=same.astype(B)
    kf=key.astype(F)
    hi,lo=split(kf*kf)
    ss=dg(hi,ones,NN)+dg(lo,ones,NN)
    unit=kf*lax.rsqrt(ss+1e-6)
    pre=dec.astype(F)+base+shift
    ld=-0.6065306597126334/(1.0+jnp.exp(-pre))
    rem=unit/(1.0+jnp.exp(-learn.astype(F)))
    return kf,unit,ld,rem
def chunk_cum(ld):
    r,c,same=consts()
    tri=(same&(r>=c)).astype(B)
    outs=[]
    for i in range(ld.shape[0]//128):
        hi,lo=split(ld[i*128:(i+1)*128])
        outs.append(dg(tri,hi,NN)+dg(tri,lo,NN))
    return jnp.concatenate(outs,0)
def chunk(rec,kf,vb,unit,rem,ld,cum):
    r,c,same=consts()
    lane=lax.broadcasted_iota(jnp.int32,(C,128),1)
    m0=lane<64
    mid=cum[C//2-1:C//2]; end=cum[C-1:C]
    rel=cum-mid
    Q=rec*jnp.exp(rel); P=unit*jnp.exp(rel-ld)
    sh=jnp.exp(-rel)
    BR=(rem*sh).astype(B); BK=(kf*sh).astype(B)
    Qb=Q.astype(B); Pb=P.astype(B)
    z=jnp.zeros((C,128),B)
    ex=lambda x: jnp.concatenate([jnp.where(m0,x,z),jnp.where(m0,z,x)],0)
    Pe=ex(Pb)
    lhs=jnp.concatenate([Pe,ex(Qb)],0)
    sR=dg(lhs,jnp.concatenate([BR,BR],0),NT)
    sK=dg(lhs,jnp.concatenate([BK,BK],0),NT)
    yield None
    strict=same&(r>c); incl=same&(r>=c)
    zf=jnp.zeros((128,128),F)
    A=jnp.where(strict,sR[:128],zf).astype(B)
    PK=jnp.where(strict,sK[:128],zf).astype(B)
    QR=jnp.where(incl,sR[128:],zf).astype(B)
    QK=jnp.where(incl,sK[128:],zf).astype(B)
    zb=jnp.zeros((128,128),B)
    x=r^c
    lm=lambda m: (x>=m)&(x<2*m)
    D=jnp.where(r==c,1.0,0.0).astype(B)-jnp.where(lm(1),A,zb)
    m=2
    while m<C:
        E=dg(jnp.where(lm(m),A,zb),D,NN).astype(B)
        yield None
        D=D-dg(D,E,NN).astype(B)
        yield None
        m*=2
    Ve=ex(vb)
    kv=dg(jnp.concatenate([PK,QK],0),Ve,NN)
    yield None
    X=dg(D,jnp.concatenate([Pe,kv[:128].astype(B)],1),NN)
    Xb=X.astype(B)
    yield None
    qx=dg(QR,Xb,NN)
    yield None
    em=jnp.exp(mid); et=jnp.exp(end-mid)
    reader=(Q-fold(qx[:,:128],C))*em
    local=fold(kv[128:],C)-fold(qx[:,128:],C)
    X0=fold(Xb[:,:128],C); L=fold(Xb[:,128:],C)
    tx=dg(X0,BR,TN)
    yield None
    eye=jnp.where(r==c,1.0,0.0).astype(F)
    emT=jnp.sum(jnp.where(r==c,jnp.broadcast_to(em,(128,128)),zf),1,keepdims=True)
    T=jnp.where(same,(eye-tx)*emT*et,zf)
    off=dg(jnp.concatenate([vb,-L],0),jnp.concatenate([BK,BR],0),TN)
    off=jnp.where(same,off*et,zf)
    yield reader,local,T,off
def local_scan(rec,key,val,dec,learn,base,shift):
    n=key.shape[0]//C
    kf,unit,ld,rem=pre_stage(key,dec,learn,base,shift)
    cum=chunk_cum(ld)
    outs=[]
    for i in range(n):
        s=slice(i*C,(i+1)*C)
        outs.append(chunk(rec[s].astype(F),kf[s],val[s],unit[s],rem[s],ld[s],cum[s]))
    while True:
        now=[next(o) for o in outs]
        if now[0] is not None: break
    outs=now
    r,c,same=consts()
    PB=None
    rd=[];lc=[]
    for i in range(n):
        reader,local,T,off=outs[i]
        if PB is None:
            rd.append(reader); lc.append(local)
            PB=jnp.concatenate([T,off],0)
        else:
            ph,pl_=split(PB)
            rh=reader.astype(B)
            q=dg(rh,ph,NT)
            rd.append(q[:,:128]); lc.append(local+q[:,128:])
            PB=dot3(PB,T,NN)+jnp.concatenate([jnp.zeros_like(off),off],0)
    return jnp.concatenate(rd,0),jnp.concatenate(lc,0),PB[:128],PB[128:]


def spread(compact):
    lane = lax.broadcasted_iota(jnp.int32, compact.shape, 1)
    nil = jnp.zeros_like(compact)
    return jnp.concatenate([jnp.where(lane < 64, compact, nil), jnp.where(lane < 64, nil, compact)], 0)


def unpack(message):
    r, c, same = consts()
    eye = jnp.where(r == c, 1.0, 0.0).astype(F)
    wide = message.astype(F)
    return spread(wide[:C]) + eye, wide[C:]


def head_sum(x, ones):
    hi, lo = split(x)
    return dg(hi, ones, NN) + dg(lo, ones, NN)


def remote(src, dst, send, recv, where):
    return pltpu.make_async_remote_copy(
        src_ref=src, dst_ref=dst, send_sem=send, recv_sem=recv, device_id=where, device_id_type=MESH
    )


def wait_bytes(ref, sem):
    pltpu.make_async_copy(ref, ref, sem).wait()


def kernel(
    rec_hbm, key_hbm, val_hbm, dec_hbm, learn_hbm, wout_hbm, x_hbm, gate_hbm, up_hbm, down_hbm,
    base_ref, shift_ref, gain_ref, xgain_ref, routes_ref, rw_ref,
    mixer_ref, expert_ref,
    mix_in, wout, xin, g_buf, u_buf, d_buf, rd_buf, lc_buf, mb_buf, row_buf, exc_buf, tz_buf, z_buf, fin_buf, st_buf,
    wt_buf, out_buf, arr_buf, acc, hid_buf, res_buf, ret_buf, part_buf, rs_buf,
    in_sems, ws, wr, s1, r1, s2, r2, s3, r3, s4, misc,
):
    ep, tp = lax.axis_index("ep"), lax.axis_index("tp")
    z, m = ep // 8, ep % 8
    x, core = m // 2, m % 2
    n = 64
    mate, across = tp + 1 - 2 * (tp % 2), 3 - tp
    other = 1 - 2 * core
    prime = core == tp // 2
    client = jnp.where(prime, tp, across)
    serves = jnp.where(prime, ep, ep + other)

    loads = [pltpu.make_async_copy(x_hbm, xin, in_sems.at[0])]
    for i, src in enumerate((rec_hbm, key_hbm, val_hbm, dec_hbm, learn_hbm)):
        loads.append(pltpu.make_async_copy(src, mix_in.at[i], in_sems.at[i + 1]))
    loads.append(pltpu.make_async_copy(wout_hbm, wout, in_sems.at[6]))
    for load in loads:
        load.start()

    barrier = pltpu.get_barrier_semaphore()

    @pl.loop(1, n)
    def _(d):
        pl.semaphore_signal(barrier, inc=1, device_id={"ep": (ep + d) % n}, device_id_type=MESH)

    @pl.loop(0, n)
    def _(d):
        there = {"ep": (ep + d) % n, "tp": across}
        pl.semaphore_signal(barrier, inc=1, device_id=there, device_id_type=MESH)

    for there in (mate, 3 - mate):
        pl.semaphore_signal(barrier, inc=1, device_id={"tp": there}, device_id_type=MESH)
    pl.semaphore_wait(barrier, 2 * n + 1)

    pieces = ((gate_hbm, g_buf), (up_hbm, u_buf), (down_hbm, d_buf))
    sibling = {"ep": ep + other}

    def put(src, i, slot, sem, where):
        remote(src, pieces[i][1].at[slot], ws.at[sem], wr.at[3 * slot + i], where).start()

    def land(i, slot):
        wait_bytes(pieces[i][1].at[slot], wr.at[3 * slot + i])

    def hop(i):
        @pl.when(prime)
        def _():
            land(i, 2)
            put(pieces[i][1].at[2], i, 3, 6 + i, {"tp": mate})
            put(pieces[i][1].at[2], i, 2, 9 + i, sibling)

    def share(i, slot):
        @pl.when(prime)
        def _():
            land(i, slot)
            put(pieces[i][1].at[slot], i, slot, 12 + 3 * (slot // 3) + i, sibling)

    def others_land(i, slot):
        @pl.when(jnp.logical_not(prime))
        def _():
            land(i, slot)

    @pl.when(prime)
    def _():
        for i, (src, dst) in enumerate(pieces):
            put(src, i, 1, i, {"tp": mate})
        for i, (src, dst) in enumerate(pieces):
            put(src, i, 0, 3 + i, sibling)
            pltpu.make_async_copy(src, dst.at[0], wr.at[i]).start()

    @pl.when(jnp.logical_not(prime))
    def _():
        for i, (src, dst) in enumerate(pieces):
            put(src, i, 2, i, {"tp": across})

    loads[0].wait()
    rows = xin[...].astype(F)
    normed = (rows * lax.rsqrt(jnp.mean(rows * rows, axis=1, keepdims=True) + NORM_EPS) * xgain_ref[...]).astype(B)
    r0, r1_ = routes_ref[0:1, :], routes_ref[1:2, :]
    r, c, same = consts()
    hits = ((r == r0) | (r == r1_)).astype(F).astype(B)
    earlier = dg(hits, (r < c).astype(F).astype(B), NN)
    t0 = r0.astype(F) * 8.0 + jnp.sum(jnp.where(r == r0, earlier, 0.0), 0, keepdims=True)
    t1 = r1_.astype(F) * 8.0 + jnp.sum(jnp.where(r == r1_, earlier, 0.0), 0, keepdims=True)
    place = lax.broadcasted_iota(jnp.int32, (n * 8, 128), 0).astype(F)
    first, second = place == t0, place == t1
    marks = jnp.where(first | second, 1.0, 0.0).astype(B)
    hi, lo = split(jnp.where(first, rw_ref[0:1, :], 0.0) + jnp.where(second, rw_ref[1:2, :], 0.0))
    wt_buf[0] = hi
    wt_buf[1] = lo
    for b in range(4):
        out_buf[16 * b : 16 * b + 16] = (
            dg(marks[128 * b : 128 * b + 128], normed, NN).reshape(16, 8, -1).astype(B)
        )

    def dispatch(e):
        differ = (e % 2 + tp // 2) % 2
        there = {"ep": e + differ * (1 - 2 * (e % 2)), "tp": tp + differ * (3 - 2 * tp)}
        remote(out_buf.at[e], arr_buf.at[ep], s4.at[0], s4.at[1], there).start()

    @pl.loop(0, n // 2)
    def _(d):
        dispatch((ep + 2 * d + 1) % n)

    for load in loads[1:6]:
        load.wait()

    high, rest = split(shift_ref[...])
    middle, low = split(shift_ref[...] - high.astype(F))
    shifts = jnp.concatenate([high.astype(F), middle.astype(F), low.astype(F)], 0).astype(B)

    @pl.loop(0, 4)
    def _(p):
        lanes = pl.ds(pl.multiple_of(p * 128, 128), 128)
        head = lax.broadcasted_iota(jnp.int32, (24, 128), 0) % 8
        lane = lax.broadcasted_iota(jnp.int32, (24, 128), 1)
        shift = dg(shifts, (head == 2 * p + lane // 64).astype(F).astype(B), TN)
        a = [mix_in[i, :, lanes] for i in range(5)]
        rd, lc, whole, offset = local_scan(*a, base_ref[:, lanes], shift)
        rd_buf[:, lanes] = rd.astype(B)
        lc_buf[:, lanes] = lc
        r, c, same = consts()
        less = fold(whole - jnp.where(r == c, 1.0, 0.0), C)
        mb_buf[p] = jnp.concatenate([less, fold(offset, C)], 0).astype(B)

    def row_copy(d, slot):
        j = (m + d) % 8
        return remote(mb_buf.at[j // 2], row_buf.at[slot], s1.at[d], r1.at[slot], {"ep": z * 8 + j})

    for d in range(1, 8):
        row_copy(d, m).start()

    hop(0)
    row_buf[m] = mb_buf[x]
    for d in range(1, 8):
        row_copy(d, (m + d) % 8).wait_recv()
    eye = fold(jnp.where(r == c, 1.0, 0.0).astype(F), C)
    none = jnp.zeros((C, 128), F)
    running = jnp.concatenate([eye, none], 0)
    for j in range(8):
        exc_buf[j] = running
        step, offset = unpack(row_buf[j])
        if j == 0:
            running = jnp.concatenate([fold(step, C), offset], 0)
        else:
            running = dot3(running, step, NN) + jnp.concatenate([none, offset], 0)
    tz_buf[...] = (running - jnp.concatenate([eye, none], 0)).astype(B)

    def z_copy(d, slot):
        return remote(tz_buf, z_buf.at[slot], s2.at[d], r2.at[slot], {"ep": ((z + d) % 8) * 8 + m})

    for d in range(1, 8):
        z_copy(d, z).start()

    @pl.when(prime)
    def _():
        pltpu.make_async_copy(out_buf.at[ep], arr_buf.at[ep], s4.at[1]).start()

    @pl.when(jnp.logical_not(prime))
    def _():
        dispatch(ep)

    @pl.loop(1, n // 2)
    def _(d):
        dispatch((ep + 2 * d) % n)

    hop(1)
    z_buf[z] = tz_buf[...]
    for d in range(1, 8):
        z_copy(d, (z + d) % 8).wait_recv()
    state = none
    for j in range(7):
        step, offset = unpack(z_buf[j])
        after = offset if j == 0 else dot3(state, step, NN) + offset
        state = jnp.where(j < z, after, state)
    for k in range(4):
        member = exc_buf[k * 2 + core]
        fin_buf[k] = (dot3(state, spread(member[:C]), NN) + member[C:]).astype(B)

    def fin_copy(d, slot):
        k = (x + d) % 4
        return remote(fin_buf.at[k], st_buf.at[slot], s3.at[d], r3.at[slot], {"ep": z * 8 + k * 2 + core})

    for d in range(1, 4):
        fin_copy(d, x).start()

    hop(2)
    st_buf[x] = fin_buf[x]
    for d in range(1, 4):
        fin_copy(d, (x + d) % 4).wait_recv()

    loads[6].wait()
    ones = jnp.where(same, 1.0 / 64, 0.0).astype(B)
    for b in range(4):
        here = slice(128 * b, 128 * b + 128)
        parts = []
        for p in range(4):
            lanes = slice(p * 128, (p + 1) * 128)
            read = lc_buf[here, lanes] + dg(rd_buf[here, lanes], spread(st_buf[p]), NT)
            centred = read - head_sum(read, ones)
            variance = head_sum(centred * centred, ones)
            parts.append((centred * lax.rsqrt(variance + GROUP_EPS) * gain_ref[:, lanes]).astype(B))
        part_buf[b] = dg(jnp.concatenate(parts, 1), wout[...], NN).astype(B)

    for i in range(3):
        share(i, 1)
    wait_bytes(arr_buf, s4.at[1])

    def hidden(s, b):
        given = arr_buf[pl.ds(16 * b, 16)].reshape(128, -1)
        gate = dg(given, g_buf[s], NN)
        up = dg(given, u_buf[s], NN)
        return (gate / (1.0 + jnp.exp(-gate)) * up).astype(B)

    def units(s, b):
        return dg(hidden(s, b), d_buf[s], NN)

    def rows_of(b):
        return pl.ds(pl.multiple_of(b * 128, 128), 128)

    for i in range(3):
        land(i, 0)

    @pl.loop(0, 4)
    def _(b):
        acc[rows_of(b), :] = units(0, b)

    for slot in (1, 2):
        for i in range(3):
            others_land(i, slot)

        @pl.loop(0, 4)
        def _(b):
            acc[rows_of(b), :] += units(slot, b)

    for i in range(2):
        share(i, 3)
        others_land(i, 3)

    @pl.loop(0, 4)
    def _(b):
        hid_buf[rows_of(b), :] = hidden(3, b)

    share(2, 3)
    others_land(2, 3)

    @pl.loop(0, 4)
    def _(i):
        b = (z // 2 + i) % 4
        res_buf[pl.ds(16 * b, 16)] = (
            (acc[rows_of(b), :] + dg(hid_buf[rows_of(b), :], d_buf[3], NN)).reshape(16, 8, -1).astype(B)
        )

        @pl.loop(0, 16)
        def _(k):
            there = 16 * b + (ep + k) % 16

            @pl.when(jnp.logical_or(there != ep, jnp.logical_not(prime)))
            def _():
                where = {"ep": there, "tp": client}
                remote(res_buf.at[there], ret_buf.at[serves], misc.at[0], misc.at[1], where).start()

    @pl.when(prime)
    def _():
        pltpu.make_async_copy(res_buf.at[ep], ret_buf.at[ep], misc.at[1]).start()

    def rs_copy(d, slot):
        j = (tp + d) % 4
        return remote(part_buf.at[j], rs_buf.at[slot], ws.at[17 + d], wr.at[12 + slot], {"tp": j})

    for d in range(1, 4):
        rs_copy(d, tp).start()
    total = part_buf[tp].astype(F)
    for d in range(1, 4):
        rs_copy(d, (tp + d) % 4).wait_recv()
        total += rs_buf[(tp + d) % 4].astype(F)
    mixer_ref[...] = total.astype(B)

    wait_bytes(ret_buf, misc.at[1])
    back_rows = ret_buf[...].reshape(n * 8, -1)
    expert_ref[...] = (dg(wt_buf[0], back_rows, TN) + dg(wt_buf[1], back_rows, TN)).astype(B)

    for d in range(1, 8):
        row_copy(d, m).wait_send()
        z_copy(d, z).wait_send()
    for d in range(1, 4):
        fin_copy(d, x).wait_send()
        rs_copy(d, tp).wait_send()

    def sent(count, rows_sent):
        for k in range(count):
            wait_bytes(pieces[k % 3][1].at[0], ws.at[k])
        wait_bytes(out_buf.at[pl.ds(0, rows_sent)], s4.at[0])
        wait_bytes(res_buf.at[pl.ds(0, rows_sent)], misc.at[0])

    @pl.when(prime)
    def _():
        sent(18, n - 1)

    @pl.when(jnp.logical_not(prime))
    def _():
        sent(3, n)


def on_device(
    receptance, key_rows, value_rows, decay_input, learn_input, decay_base, decay_shift, channel_gain,
    out_weight, expert_input, expert_gain, routes, route_weight, gate_weight, up_weight, down_weight,
):
    t, width = expert_input.shape
    rows, channels = receptance.shape
    depth, units = gate_weight.shape[1:]
    vmem = pl.BlockSpec(memory_space=pltpu.VMEM)
    anywhere = pl.BlockSpec(memory_space=pl.ANY)
    dma = pltpu.SemaphoreType.DMA
    V = pltpu.VMEM
    return pl.pallas_call(
        kernel,
        in_specs=[anywhere] * 10 + [vmem] * 6,
        out_specs=[vmem, vmem],
        out_shape=[jax.ShapeDtypeStruct((t, width), B)] * 2,
        scratch_shapes=[
            V((5, rows, channels), B), V((channels, width), B), V((t, width), B),
            V((4, depth, units), B), V((4, depth, units), B), V((4, units, width), B),
            V((rows, channels), B), V((rows, channels), F),
            V((4, 128, 128), B), V((8, 128, 128), B), V((8, 128, 128), F), V((128, 128), B), V((8, 128, 128), B),
            V((4, C, 128), B), V((4, C, 128), B),
            V((2, 512, t), B), V((64, 8, width), B), V((64, 8, width), B), V((512, width), F), V((512, units), B),
            V((64, 8, width), B), V((64, 8, width), B), V((4, t, width), B), V((4, t, width), B),
            dma((7,)), dma((21,)), dma((16,)), dma((8,)), dma((8,)), dma((8,)), dma((8,)), dma((4,)), dma((4,)),
            dma((2,)), dma((2,)),
        ],
        compiler_params=pltpu.CompilerParams(
            collective_id=0, has_side_effects=True, vmem_limit_bytes=60 * 1024 * 1024
        ),
        name="step",
    )(
        receptance, key_rows, value_rows, decay_input, learn_input, out_weight, expert_input,
        gate_weight[0], up_weight[0], down_weight[0],
        decay_base.reshape(1, channels), decay_shift.T, channel_gain.reshape(1, channels), expert_gain.reshape(1, width),
        routes.T, route_weight.T,
    )


def solution(mesh):
    both = P(("ep", "tp"), None)
    placed = (
        P("ep", "tp"), P("ep", "tp"), P("ep", "tp"), P("ep", "tp"), P("ep", "tp"), P("tp"), P("ep", "tp"), P("tp"),
        P("tp", None), both, P(), both, both, P("ep", None, "tp"), P("ep", None, "tp"), P("ep", "tp", None),
    )
    return jax.shard_map(on_device, mesh=mesh, in_specs=placed, out_specs=(both, both), check_vma=False)
```

```python
import functools

import jax
import jax.numpy as jnp
from jax import lax
from jax.experimental import pallas as pl
from jax.experimental.pallas import tpu as pltpu
from jax.sharding import PartitionSpec as P


MESH = pl.DeviceIdType.MESH
NORM_EPS = 1e-06
GROUP_EPS = 0.00064
F=jnp.float32; B=jnp.bfloat16
C=64
NT=(((1,),(1,)),((),())); NN=(((1,),(0,)),((),())); TN=(((0,),(0,)),((),()))
def dg(a,b,dims): return lax.dot_general(a,b,dims,preferred_element_type=F)
def split(x):
    hi=x.astype(B); return hi,(x-hi.astype(F)).astype(B)
def dot3(a,b,dims):
    ah,al=split(a); bh,bl=split(b)
    return dg(ah,bh,dims)+(dg(ah,bl,dims)+dg(al,bh,dims))
def fold(x,n): return x[:n]+x[n:]
def consts():
    r=lax.broadcasted_iota(jnp.int32,(128,128),0); c=lax.broadcasted_iota(jnp.int32,(128,128),1)
    same=(r//64)==(c//64)
    return r,c,same
def pre_stage(key,dec,learn,base,shift):
    r,c,same=consts()
    ones=same.astype(B)
    kf=key.astype(F)
    hi,lo=split(kf*kf)
    ss=dg(hi,ones,NN)+dg(lo,ones,NN)
    unit=kf*lax.rsqrt(ss+1e-6)
    pre=dec.astype(F)+base+shift
    ld=-0.6065306597126334/(1.0+jnp.exp(-pre))
    rem=unit/(1.0+jnp.exp(-learn.astype(F)))
    return kf,unit,ld,rem
def chunk_cum(ld):
    r,c,same=consts()
    tri=(same&(r>=c)).astype(B)
    outs=[]
    for i in range(ld.shape[0]//128):
        hi,lo=split(ld[i*128:(i+1)*128])
        outs.append(dg(tri,hi,NN)+dg(tri,lo,NN))
    return jnp.concatenate(outs,0)
def chunk(rec,kf,vb,unit,rem,ld,cum):
    r,c,same=consts()
    lane=lax.broadcasted_iota(jnp.int32,(C,128),1)
    m0=lane<64
    mid=cum[C//2-1:C//2]; end=cum[C-1:C]
    rel=cum-mid
    Q=rec*jnp.exp(rel); P=unit*jnp.exp(rel-ld)
    sh=jnp.exp(-rel)
    BR=(rem*sh).astype(B); BK=(kf*sh).astype(B)
    Qb=Q.astype(B); Pb=P.astype(B)
    z=jnp.zeros((C,128),B)
    ex=lambda x: jnp.concatenate([jnp.where(m0,x,z),jnp.where(m0,z,x)],0)
    Pe=ex(Pb)
    lhs=jnp.concatenate([Pe,ex(Qb)],0)
    sR=dg(lhs,jnp.concatenate([BR,BR],0),NT)
    sK=dg(lhs,jnp.concatenate([BK,BK],0),NT)
    yield None
    strict=same&(r>c); incl=same&(r>=c)
    zf=jnp.zeros((128,128),F)
    A=jnp.where(strict,sR[:128],zf).astype(B)
    PK=jnp.where(strict,sK[:128],zf).astype(B)
    QR=jnp.where(incl,sR[128:],zf).astype(B)
    QK=jnp.where(incl,sK[128:],zf).astype(B)
    zb=jnp.zeros((128,128),B)
    x=r^c
    lm=lambda m: (x>=m)&(x<2*m)
    D=jnp.where(r==c,1.0,0.0).astype(B)-jnp.where(lm(1),A,zb)
    m=2
    while m<C:
        E=dg(jnp.where(lm(m),A,zb),D,NN).astype(B)
        yield None
        D=D-dg(D,E,NN).astype(B)
        yield None
        m*=2
    Ve=ex(vb)
    kv=dg(jnp.concatenate([PK,QK],0),Ve,NN)
    yield None
    X=dg(D,jnp.concatenate([Pe,kv[:128].astype(B)],1),NN)
    Xb=X.astype(B)
    yield None
    qx=dg(QR,Xb,NN)
    yield None
    em=jnp.exp(mid); et=jnp.exp(end-mid)
    reader=(Q-fold(qx[:,:128],C))*em
    local=fold(kv[128:],C)-fold(qx[:,128:],C)
    X0=fold(Xb[:,:128],C); L=fold(Xb[:,128:],C)
    tx=dg(X0,BR,TN)
    yield None
    eye=jnp.where(r==c,1.0,0.0).astype(F)
    emT=jnp.sum(jnp.where(r==c,jnp.broadcast_to(em,(128,128)),zf),1,keepdims=True)
    T=jnp.where(same,(eye-tx)*emT*et,zf)
    off=dg(jnp.concatenate([vb,-L],0),jnp.concatenate([BK,BR],0),TN)
    off=jnp.where(same,off*et,zf)
    yield reader,local,T,off
def local_scan(rec,key,val,dec,learn,base,shift):
    n=key.shape[0]//C
    kf,unit,ld,rem=pre_stage(key,dec,learn,base,shift)
    cum=chunk_cum(ld)
    outs=[]
    for i in range(n):
        s=slice(i*C,(i+1)*C)
        outs.append(chunk(rec[s].astype(F),kf[s],val[s],unit[s],rem[s],ld[s],cum[s]))
    while True:
        now=[next(o) for o in outs]
        if now[0] is not None: break
    outs=now
    r,c,same=consts()
    PB=None
    rd=[];lc=[]
    for i in range(n):
        reader,local,T,off=outs[i]
        if PB is None:
            rd.append(reader); lc.append(local)
            PB=jnp.concatenate([T,off],0)
        else:
            ph,pl_=split(PB)
            rh=reader.astype(B)
            q=dg(rh,ph,NT)
            rd.append(q[:,:128]); lc.append(local+q[:,128:])
            PB=dot3(PB,T,NN)+jnp.concatenate([jnp.zeros_like(off),off],0)
    return jnp.concatenate(rd,0),jnp.concatenate(lc,0),PB[:128],PB[128:]


def spread(compact):
    lane = lax.broadcasted_iota(jnp.int32, compact.shape, 1)
    nil = jnp.zeros_like(compact)
    return jnp.concatenate([jnp.where(lane < 64, compact, nil), jnp.where(lane < 64, nil, compact)], 0)


def unpack(message):
    r, c, same = consts()
    eye = jnp.where(r == c, 1.0, 0.0).astype(F)
    wide = message.astype(F)
    return spread(wide[:C]) + eye, wide[C:]


def head_sum(x, ones):
    hi, lo = split(x)
    return dg(hi, ones, NN) + dg(lo, ones, NN)


def places(routes_ref, experts):
    r0, r1 = routes_ref[0:1, :], routes_ref[1:2, :]
    r, c, same = consts()
    hits = ((r == r0) | (r == r1)).astype(F).astype(B)
    earlier = dg(hits, (r < c).astype(F).astype(B), NN)
    t0 = r0.astype(F) * 8.0 + jnp.sum(jnp.where(r == r0, earlier, 0.0), 0, keepdims=True)
    t1 = r1.astype(F) * 8.0 + jnp.sum(jnp.where(r == r1, earlier, 0.0), 0, keepdims=True)
    place = lax.broadcasted_iota(jnp.int32, (experts * 8, 128), 0).astype(F)
    return place == t0, place == t1


def remote(src, dst, send, recv, where):
    return pltpu.make_async_remote_copy(
        src_ref=src, dst_ref=dst, send_sem=send, recv_sem=recv, device_id=where, device_id_type=MESH
    )


def wait_bytes(ref, sem):
    pltpu.make_async_copy(ref, ref, sem).wait()


def kernel(
    rec_hbm, key_hbm, val_hbm, dec_hbm, learn_hbm, wout_hbm, x_hbm, gate_hbm, up_hbm, down_hbm,
    base_ref, shift_ref, gain_ref, xgain_ref, routes_ref,
    mixer_ref, ret_buf,
    mix_in, wout, xin, g_buf, u_buf, d_buf, rd_buf, lc_buf, mb_buf, row_buf, exc_buf, tz_buf, z_buf, fin_buf, st_buf,
    out_buf, arr_buf, acc, hid_buf, res_buf, part_buf, rs_buf,
    in_sems, ws, wr, s1, r1, s2, r2, s3, r3, s4, misc,
):
    ep, tp = lax.axis_index("ep"), lax.axis_index("tp")
    z, m = ep // 8, ep % 8
    x, core = m // 2, m % 2
    n = 64
    mate, across = tp + 1 - 2 * (tp % 2), 3 - tp
    other = 1 - 2 * core
    prime = core == tp // 2
    client = jnp.where(prime, tp, across)
    serves = jnp.where(prime, ep, ep + other)

    loads = [pltpu.make_async_copy(x_hbm, xin, in_sems.at[0])]
    for i, src in enumerate((rec_hbm, key_hbm, val_hbm, dec_hbm, learn_hbm)):
        loads.append(pltpu.make_async_copy(src, mix_in.at[i], in_sems.at[i + 1]))
    loads.append(pltpu.make_async_copy(wout_hbm, wout, in_sems.at[6]))
    for load in loads:
        load.start()

    barrier = pltpu.get_barrier_semaphore()

    @pl.loop(1, n, unroll=9)
    def _(d):
        pl.semaphore_signal(barrier, inc=1, device_id={"ep": (ep + d) % n}, device_id_type=MESH)

    @pl.loop(0, n, unroll=8)
    def _(d):
        there = {"ep": (ep + d) % n, "tp": across}
        pl.semaphore_signal(barrier, inc=1, device_id=there, device_id_type=MESH)

    for there in (mate, 3 - mate):
        pl.semaphore_signal(barrier, inc=1, device_id={"tp": there}, device_id_type=MESH)
    loads[0].wait()
    rows = xin[...].astype(F)
    normed = (rows * lax.rsqrt(jnp.mean(rows * rows, axis=1, keepdims=True) + NORM_EPS) * xgain_ref[...]).astype(B)
    first, second = places(routes_ref, n)
    marks = jnp.where(first | second, 1.0, 0.0).astype(B)
    r, c, same = consts()
    for b in range(4):
        out_buf[16 * b : 16 * b + 16] = (
            dg(marks[128 * b : 128 * b + 128], normed, NN).reshape(16, 8, -1).astype(B)
        )

    pl.semaphore_wait(barrier, 2 * n + 1)

    pieces = ((gate_hbm, g_buf), (up_hbm, u_buf), (down_hbm, d_buf))
    sibling = {"ep": ep + other}

    def put(src, i, slot, sem, where):
        remote(src, pieces[i][1].at[slot], ws.at[sem], wr.at[3 * slot + i], where).start()

    def land(i, slot):
        wait_bytes(pieces[i][1].at[slot], wr.at[3 * slot + i])

    half = d_buf.shape[1] // 2
    halves = (pl.ds(0, half), pl.ds(half, half))

    def last(src, h, sem, where):
        remote(src, d_buf.at[3, halves[h]], ws.at[sem], wr.at[(11, 16)[h]], where).start()

    def last_land(h):
        wait_bytes(d_buf.at[3, halves[h]], wr.at[(11, 16)[h]])

    def hop(i):
        @pl.when(prime)
        def _():
            land(i, 2)
            if i < 2:
                put(pieces[i][1].at[2], i, 3, 6 + i, {"tp": mate})
            else:
                for h in range(2):
                    last(d_buf.at[2, halves[h]], h, (8, 21)[h], {"tp": mate})
            put(pieces[i][1].at[2], i, 2, 9 + i, sibling)

    def share(i, slot):
        @pl.when(prime)
        def _():
            land(i, slot)
            put(pieces[i][1].at[slot], i, slot, 12 + 3 * (slot // 3) + i, sibling)

    def others_land(i, slot):
        @pl.when(jnp.logical_not(prime))
        def _():
            land(i, slot)

    @pl.when(prime)
    def _():
        for i, (src, dst) in enumerate(pieces):
            put(src, i, 1, i, {"tp": mate})
        for i, (src, dst) in enumerate(pieces):
            put(src, i, 0, 3 + i, sibling)
            pltpu.make_async_copy(src, dst.at[0], wr.at[i]).start()

    @pl.when(jnp.logical_not(prime))
    def _():
        for i, (src, dst) in enumerate(pieces):
            put(src, i, 2, i, {"tp": across})

    def dispatch(e):
        differ = (e % 2 + tp // 2) % 2
        there = {"ep": e + differ * (1 - 2 * (e % 2)), "tp": tp + differ * (3 - 2 * tp)}
        remote(out_buf.at[e], arr_buf.at[ep], s4.at[0], s4.at[1], there).start()

    @pl.loop(0, n // 2)
    def _(d):
        dispatch((ep + 2 * d + 1) % n)

    for load in loads[1:6]:
        load.wait()

    high, rest = split(shift_ref[...])
    middle, low = split(shift_ref[...] - high.astype(F))
    shifts = jnp.concatenate([high.astype(F), middle.astype(F), low.astype(F)], 0).astype(B)

    @pl.loop(0, 4)
    def _(p):
        lanes = pl.ds(pl.multiple_of(p * 128, 128), 128)
        head = lax.broadcasted_iota(jnp.int32, (24, 128), 0) % 8
        lane = lax.broadcasted_iota(jnp.int32, (24, 128), 1)
        shift = dg(shifts, (head == 2 * p + lane // 64).astype(F).astype(B), TN)
        a = [mix_in[i, :, lanes] for i in range(5)]
        rd, lc, whole, offset = local_scan(*a, base_ref[:, lanes], shift)
        rd_buf[:, lanes] = rd.astype(B)
        lc_buf[:, lanes] = lc
        r, c, same = consts()
        less = fold(whole - jnp.where(r == c, 1.0, 0.0), C)
        mb_buf[p] = jnp.concatenate([less, fold(offset, C)], 0).astype(B)

    def row_copy(d, slot):
        j = (m + d) % 8
        return remote(mb_buf.at[j // 2], row_buf.at[slot], s1.at[d], r1.at[slot], {"ep": z * 8 + j})

    for d in range(1, 8):
        row_copy(d, m).start()

    @pl.loop(1, n // 4)
    def _(d):
        dispatch((ep + 4 * d) % n)

    hop(0)
    row_buf[m] = mb_buf[x]
    for d in range(1, 8):
        row_copy(d, (m + d) % 8).wait_recv()
    eye = fold(jnp.where(r == c, 1.0, 0.0).astype(F), C)
    none = jnp.zeros((C, 128), F)
    running = jnp.concatenate([eye, none], 0)
    for j in range(8):
        exc_buf[j] = running
        step, offset = unpack(row_buf[j])
        if j == 0:
            running = jnp.concatenate([fold(step, C), offset], 0)
        else:
            running = dot3(running, step, NN) + jnp.concatenate([none, offset], 0)
    tz_buf[...] = (running - jnp.concatenate([eye, none], 0)).astype(B)

    def z_copy(d, slot):
        return remote(tz_buf, z_buf.at[slot], s2.at[d], r2.at[slot], {"ep": ((z + d) % 8) * 8 + m})

    for d in range(1, 8):
        z_copy(d, z).start()

    @pl.when(prime)
    def _():
        pltpu.make_async_copy(out_buf.at[ep], arr_buf.at[ep], s4.at[1]).start()

    @pl.when(jnp.logical_not(prime))
    def _():
        dispatch(ep)

    @pl.loop(0, n // 4)
    def _(d):
        dispatch((ep + 4 * d + 2) % n)

    hop(1)
    for i in range(3):
        share(i, 1)
    z_buf[z] = tz_buf[...]
    for d in range(1, 8):
        z_copy(d, (z + d) % 8).wait_recv()
    state = none
    for j in range(7):
        step, offset = unpack(z_buf[j])
        after = offset if j == 0 else dot3(state, step, NN) + offset
        state = jnp.where(j < z, after, state)
    for k in range(4):
        member = exc_buf[k * 2 + core]
        fin_buf[k] = (dot3(state, spread(member[:C]), NN) + member[C:]).astype(B)

    def fin_copy(d, slot):
        k = (x + d) % 4
        return remote(fin_buf.at[k], st_buf.at[slot], s3.at[d], r3.at[slot], {"ep": z * 8 + k * 2 + core})

    for d in range(1, 4):
        fin_copy(d, x).start()

    st_buf[x] = fin_buf[x]
    for d in range(1, 4):
        fin_copy(d, (x + d) % 4).wait_recv()

    loads[6].wait()
    ones = jnp.where(same, 1.0 / 64, 0.0).astype(B)
    for b in range(4):
        here = slice(128 * b, 128 * b + 128)
        parts = []
        for p in range(4):
            lanes = slice(p * 128, (p + 1) * 128)
            read = lc_buf[here, lanes] + dg(rd_buf[here, lanes], spread(st_buf[p]), NT)
            centred = read - head_sum(read, ones)
            variance = head_sum(centred * centred, ones)
            parts.append((centred * lax.rsqrt(variance + GROUP_EPS) * gain_ref[:, lanes]).astype(B))
        part_buf[b] = dg(jnp.concatenate(parts, 1), wout[...], NN).astype(B)

    hop(2)
    def rs_copy(d, slot):
        j = (tp + d) % 4
        return remote(part_buf.at[j], rs_buf.at[slot], ws.at[17 + d], wr.at[12 + slot], {"tp": j})

    def rs_to(j):
        return remote(part_buf.at[j], rs_buf.at[tp], ws.at[18 + (j - tp + 3) % 4], wr.at[12 + tp], {"tp": j})

    rs_to(across).start()

    wait_bytes(arr_buf, s4.at[1])

    def hidden(s, b):
        given = arr_buf[pl.ds(16 * b, 16)].reshape(128, -1)
        gate = dg(given, g_buf[s], NN)
        up = dg(given, u_buf[s], NN)
        return (gate / (1.0 + jnp.exp(-gate)) * up).astype(B)

    def units(s, b):
        return dg(hidden(s, b), d_buf[s], NN)

    def rows_of(b):
        return pl.ds(pl.multiple_of(b * 128, 128), 128)

    for i in range(3):
        land(i, 0)

    @pl.loop(0, 4)
    def _(b):
        acc[rows_of(b), :] = units(0, b)

    def add_slot(slot):
        for i in range(3):
            others_land(i, slot)

        @pl.loop(0, 4)
        def _(b):
            acc[rows_of(b), :] += units(slot, b)

    add_slot(1)
    add_slot(2)
    for i in range(2):
        share(i, 3)
        others_land(i, 3)

    @pl.loop(0, 4)
    def _(b):
        hid_buf[rows_of(b), :] = hidden(3, b)

    for h in range(2):
        last_land(h)

        @pl.when(prime)
        def _():
            last(d_buf.at[3, halves[h]], h, (17, 22)[h], sibling)

    rs_to(mate).start()
    rs_to(3 - mate).start()

    @pl.loop(0, 4)
    def _(i):
        b = (z // 2 + 2 + i) % 4
        res_buf[pl.ds(16 * b, 16)] = (
            (acc[rows_of(b), :] + dg(hid_buf[rows_of(b), :], d_buf[3], NN)).reshape(16, 8, -1).astype(B)
        )

        @pl.loop(0, 16)
        def _(k):
            there = 16 * b + (ep + k) % 16

            @pl.when(jnp.logical_or(there != ep, jnp.logical_not(prime)))
            def _():
                where = {"ep": there, "tp": client}
                remote(res_buf.at[there], ret_buf.at[serves], misc.at[0], misc.at[1], where).start()

    @pl.when(prime)
    def _():
        pltpu.make_async_copy(res_buf.at[ep], ret_buf.at[ep], misc.at[1]).start()

    total = part_buf[tp].astype(F)
    for d in range(1, 4):
        rs_copy(d, (tp + d) % 4).wait_recv()
        total += rs_buf[(tp + d) % 4].astype(F)
    xin[...] = total.astype(B)
    leave = [pltpu.make_async_copy(xin, mixer_ref, in_sems.at[0])]
    leave[0].start()

    wait_bytes(ret_buf, misc.at[1])
    for d in range(1, 8):
        row_copy(d, m).wait_send()
        z_copy(d, z).wait_send()
    for d in range(1, 4):
        fin_copy(d, x).wait_send()
        rs_copy(d, tp).wait_send()

    def sent(count, rows_sent):
        for k in range(count):
            if k not in (8, 17):
                wait_bytes(pieces[k % 3][1].at[0], ws.at[k])
            else:
                for sem in (k, 21 + k // 17):
                    wait_bytes(d_buf.at[0, halves[0]], ws.at[sem])
        wait_bytes(out_buf.at[pl.ds(0, rows_sent)], s4.at[0])
        wait_bytes(res_buf.at[pl.ds(0, rows_sent)], misc.at[0])

    @pl.when(prime)
    def _():
        sent(18, n - 1)

    @pl.when(jnp.logical_not(prime))
    def _():
        sent(3, n)
    for copy in leave:
        copy.wait()


def finish_kernel(mixed, returned, routes_ref, rw_ref, mixer_ref, expert_ref, rows, mix, out, loaded, stored):
    count, width = rows.shape[0], rows.shape[2]
    parts = [pl.ds(width // 4 * k, width // 4) for k in range(4)]
    loads = [pltpu.make_async_copy(returned.at[:, :, p], rows.at[:, :, p], loaded.at[k]) for k, p in enumerate(parts)]
    loads.append(pltpu.make_async_copy(mixed, mix, loaded.at[4]))
    for load in loads:
        load.start()
    first, second = places(routes_ref, count)
    hi, lo = split(jnp.where(first, rw_ref[0:1, :], 0.0) + jnp.where(second, rw_ref[1:2, :], 0.0))
    stores = []
    for k, p in enumerate(parts):
        loads[k].wait()
        given = rows[:, :, p].reshape(count * 8, -1)
        out[:, p] = (dg(hi, given, TN) + dg(lo, given, TN)).astype(B)
        stores.append(pltpu.make_async_copy(out.at[:, p], expert_ref.at[:, p], stored.at[k]))
        stores[k].start()
    loads[4].wait()
    stores.append(pltpu.make_async_copy(mix, mixer_ref, stored.at[4]))
    stores[4].start()
    for store in stores:
        store.wait()


def on_device(
    receptance, key_rows, value_rows, decay_input, learn_input, decay_base, decay_shift, channel_gain,
    out_weight, expert_input, expert_gain, routes, route_weight, gate_weight, up_weight, down_weight,
):
    t, width = expert_input.shape
    rows, channels = receptance.shape
    depth, units = gate_weight.shape[1:]
    vmem = pl.BlockSpec(memory_space=pltpu.VMEM)
    anywhere = pl.BlockSpec(memory_space=pltpu.HBM)
    dma = pltpu.SemaphoreType.DMA
    V = pltpu.VMEM
    both = jax.ShapeDtypeStruct((t, width), B)
    mixed, returned = pl.pallas_call(
        kernel,
        in_specs=[anywhere] * 10 + [vmem] * 5,
        out_specs=[anywhere, anywhere],
        out_shape=[both, jax.ShapeDtypeStruct((64, 8, width), B)],
        scratch_shapes=[
            V((5, rows, channels), B), V((channels, width), B), V((t, width), B),
            V((4, depth, units), B), V((4, depth, units), B), V((4, units, width), B),
            V((rows, channels), B), V((rows, channels), F),
            V((4, 128, 128), B), V((8, 128, 128), B), V((8, 128, 128), F), V((128, 128), B), V((8, 128, 128), B),
            V((4, C, 128), B), V((4, C, 128), B),
            V((64, 8, width), B), V((64, 8, width), B), V((512, width), F), V((512, units), B),
            V((64, 8, width), B), V((4, t, width), B), V((4, t, width), B),
            dma((7,)), dma((23,)), dma((17,)), dma((8,)), dma((8,)), dma((8,)), dma((8,)), dma((4,)), dma((4,)),
            dma((2,)), dma((2,)),
        ],
        compiler_params=pltpu.CompilerParams(
            collective_id=0, has_side_effects=True, vmem_limit_bytes=60 * 1024 * 1024
        ),
        name="step",
    )(
        receptance, key_rows, value_rows, decay_input, learn_input, out_weight, expert_input,
        gate_weight[0], up_weight[0], down_weight[0],
        decay_base.reshape(1, channels), decay_shift.T, channel_gain.reshape(1, channels), expert_gain.reshape(1, width),
        routes.T,
    )
    return pl.pallas_call(
        finish_kernel,
        in_specs=[anywhere, anywhere, vmem, vmem],
        out_specs=[anywhere, anywhere],
        out_shape=[both, both],
        scratch_shapes=[V((64, 8, width), B), V((t, width), B), V((t, width), B), dma((5,)), dma((5,))],
        name="finish",
    )(mixed, returned, routes.T, route_weight.T)


def solution(mesh):
    both = P(("ep", "tp"), None)
    placed = (
        P("ep", "tp"), P("ep", "tp"), P("ep", "tp"), P("ep", "tp"), P("ep", "tp"), P("tp"), P("ep", "tp"), P("tp"),
        P("tp", None), both, P(), both, both, P("ep", None, "tp"), P("ep", None, "tp"), P("ep", "tp", None),
    )
    return jax.shard_map(on_device, mesh=mesh, in_specs=placed, out_specs=(both, both), check_vma=False)
```

```python
import functools

import jax
import jax.numpy as jnp
from jax import lax
from jax.experimental import pallas as pl
from jax.experimental.pallas import tpu as pltpu
from jax.sharding import PartitionSpec as P


MESH = pl.DeviceIdType.MESH
NORM_EPS = 1e-06
GROUP_EPS = 0.00064
F=jnp.float32; B=jnp.bfloat16
C=64
NT=(((1,),(1,)),((),())); NN=(((1,),(0,)),((),())); TN=(((0,),(0,)),((),()))
def dg(a,b,dims): return lax.dot_general(a,b,dims,preferred_element_type=F)
def split(x):
    hi=x.astype(B); return hi,(x-hi.astype(F)).astype(B)
def dot3(a,b,dims):
    ah,al=split(a); bh,bl=split(b)
    return dg(ah,bh,dims)+(dg(ah,bl,dims)+dg(al,bh,dims))
def fold(x,n): return x[:n]+x[n:]
def consts():
    r=lax.broadcasted_iota(jnp.int32,(128,128),0); c=lax.broadcasted_iota(jnp.int32,(128,128),1)
    same=(r//64)==(c//64)
    return r,c,same
def pre_stage(key,dec,learn,base,shift):
    r,c,same=consts()
    ones=same.astype(B)
    kf=key.astype(F)
    hi,lo=split(kf*kf)
    ss=dg(hi,ones,NN)+dg(lo,ones,NN)
    unit=kf*lax.rsqrt(ss+1e-6)
    pre=dec.astype(F)+base+shift
    ld=-0.6065306597126334/(1.0+jnp.exp(-pre))
    rem=unit/(1.0+jnp.exp(-learn.astype(F)))
    return kf,unit,ld,rem
def chunk_cum(ld):
    r,c,same=consts()
    tri=(same&(r>=c)).astype(B)
    outs=[]
    for i in range(ld.shape[0]//128):
        hi,lo=split(ld[i*128:(i+1)*128])
        outs.append(dg(tri,hi,NN)+dg(tri,lo,NN))
    return jnp.concatenate(outs,0)
def chunk(rec,kf,vb,unit,rem,ld,cum):
    r,c,same=consts()
    lane=lax.broadcasted_iota(jnp.int32,(C,128),1)
    m0=lane<64
    mid=cum[C//2-1:C//2]; end=cum[C-1:C]
    rel=cum-mid
    Q=rec*jnp.exp(rel); P=unit*jnp.exp(rel-ld)
    sh=jnp.exp(-rel)
    BR=(rem*sh).astype(B); BK=(kf*sh).astype(B)
    Qb=Q.astype(B); Pb=P.astype(B)
    z=jnp.zeros((C,128),B)
    ex=lambda x: jnp.concatenate([jnp.where(m0,x,z),jnp.where(m0,z,x)],0)
    Pe=ex(Pb)
    lhs=jnp.concatenate([Pe,ex(Qb)],0)
    sR=dg(lhs,jnp.concatenate([BR,BR],0),NT)
    sK=dg(lhs,jnp.concatenate([BK,BK],0),NT)
    yield None
    strict=same&(r>c); incl=same&(r>=c)
    zf=jnp.zeros((128,128),F)
    A=jnp.where(strict,sR[:128],zf).astype(B)
    PK=jnp.where(strict,sK[:128],zf).astype(B)
    QR=jnp.where(incl,sR[128:],zf).astype(B)
    QK=jnp.where(incl,sK[128:],zf).astype(B)
    zb=jnp.zeros((128,128),B)
    x=r^c
    lm=lambda m: (x>=m)&(x<2*m)
    D=jnp.where(r==c,1.0,0.0).astype(B)-jnp.where(lm(1),A,zb)
    m=2
    while m<C:
        E=dg(jnp.where(lm(m),A,zb),D,NN).astype(B)
        yield None
        D=D-dg(D,E,NN).astype(B)
        yield None
        m*=2
    Ve=ex(vb)
    kv=dg(jnp.concatenate([PK,QK],0),Ve,NN)
    yield None
    X=dg(D,jnp.concatenate([Pe,kv[:128].astype(B)],1),NN)
    Xb=X.astype(B)
    yield None
    qx=dg(QR,Xb,NN)
    yield None
    em=jnp.exp(mid); et=jnp.exp(end-mid)
    reader=(Q-fold(qx[:,:128],C))*em
    local=fold(kv[128:],C)-fold(qx[:,128:],C)
    X0=fold(Xb[:,:128],C); L=fold(Xb[:,128:],C)
    tx=dg(X0,BR,TN)
    yield None
    eye=jnp.where(r==c,1.0,0.0).astype(F)
    emT=jnp.sum(jnp.where(r==c,jnp.broadcast_to(em,(128,128)),zf),1,keepdims=True)
    T=jnp.where(same,(eye-tx)*emT*et,zf)
    off=dg(jnp.concatenate([vb,-L],0),jnp.concatenate([BK,BR],0),TN)
    off=jnp.where(same,off*et,zf)
    yield reader,local,T,off
def local_scan(rec,key,val,dec,learn,base,shift):
    n=key.shape[0]//C
    kf,unit,ld,rem=pre_stage(key,dec,learn,base,shift)
    cum=chunk_cum(ld)
    outs=[]
    for i in range(n):
        s=slice(i*C,(i+1)*C)
        outs.append(chunk(rec[s].astype(F),kf[s],val[s],unit[s],rem[s],ld[s],cum[s]))
    while True:
        now=[next(o) for o in outs]
        if now[0] is not None: break
    outs=now
    r,c,same=consts()
    PB=None
    rd=[];lc=[]
    for i in range(n):
        reader,local,T,off=outs[i]
        if PB is None:
            rd.append(reader); lc.append(local)
            PB=jnp.concatenate([T,off],0)
        else:
            ph,pl_=split(PB)
            rh=reader.astype(B)
            q=dg(rh,ph,NT)
            rd.append(q[:,:128]); lc.append(local+q[:,128:])
            PB=dot3(PB,T,NN)+jnp.concatenate([jnp.zeros_like(off),off],0)
    return jnp.concatenate(rd,0),jnp.concatenate(lc,0),PB[:128],PB[128:]


def spread(compact):
    lane = lax.broadcasted_iota(jnp.int32, compact.shape, 1)
    nil = jnp.zeros_like(compact)
    return jnp.concatenate([jnp.where(lane < 64, compact, nil), jnp.where(lane < 64, nil, compact)], 0)


def unpack(message):
    r, c, same = consts()
    eye = jnp.where(r == c, 1.0, 0.0).astype(F)
    wide = message.astype(F)
    return spread(wide[:C]) + eye, wide[C:]


def head_sum(x, ones):
    hi, lo = split(x)
    return dg(hi, ones, NN) + dg(lo, ones, NN)


def places(routes_ref, experts):
    r0, r1 = routes_ref[0:1, :], routes_ref[1:2, :]
    r, c, same = consts()
    hits = ((r == r0) | (r == r1)).astype(F).astype(B)
    earlier = dg(hits, (r < c).astype(F).astype(B), NN)
    t0 = r0.astype(F) * 8.0 + jnp.sum(jnp.where(r == r0, earlier, 0.0), 0, keepdims=True)
    t1 = r1.astype(F) * 8.0 + jnp.sum(jnp.where(r == r1, earlier, 0.0), 0, keepdims=True)
    place = lax.broadcasted_iota(jnp.int32, (experts * 8, 128), 0).astype(F)
    return place == t0, place == t1


def remote(src, dst, send, recv, where):
    return pltpu.make_async_remote_copy(
        src_ref=src, dst_ref=dst, send_sem=send, recv_sem=recv, device_id=where, device_id_type=MESH
    )


def wait_bytes(ref, sem):
    pltpu.make_async_copy(ref, ref, sem).wait()


ORDER = ((1, 7), (2, 6), (3, 5), (0, 4))


def kernel(
    rec_hbm, key_hbm, val_hbm, dec_hbm, learn_hbm, wout_hbm, x_hbm, gate_hbm, up_hbm, down_hbm,
    base_hbm, shift_hbm, gain_hbm, xgain_hbm, routes_hbm,
    mixer_ref, ret_buf,
    base_ref, shift_ref, gain_ref, xgain_ref, routes_ref,
    mix_in, wout, xin, g_buf, u_buf, d_buf, rd_buf, lc_buf, mb_buf, row_buf, exc_buf, tz_buf, z_buf, fin_buf, st_buf,
    out_buf, arr_buf, acc, hid_buf, res_buf, part_buf, rs_buf,
    in_sems, ws, wr, s1, r1, s2, r2, s3, r3, s4, misc,
):
    ep, tp = lax.axis_index("ep"), lax.axis_index("tp")
    z, m = ep // 8, ep % 8
    x, core = m // 2, m % 2
    n = 64
    mate, across = tp + 1 - 2 * (tp % 2), 3 - tp
    other = 1 - 2 * core
    prime = core == tp // 2
    client = jnp.where(prime, tp, across)
    serves = jnp.where(prime, ep, ep + other)

    smalls = ((routes_hbm, routes_ref), (xgain_hbm, xgain_ref), (base_hbm, base_ref), (shift_hbm, shift_ref), (gain_hbm, gain_ref))
    small = [pltpu.make_async_copy(src, dst, in_sems.at[7 + i]) for i, (src, dst) in enumerate(smalls)]
    loads = [pltpu.make_async_copy(x_hbm, xin, in_sems.at[0])]
    for i, src in enumerate((rec_hbm, key_hbm, val_hbm, dec_hbm, learn_hbm)):
        loads.append(pltpu.make_async_copy(src, mix_in.at[i], in_sems.at[i + 1]))
    loads.append(pltpu.make_async_copy(wout_hbm, wout, in_sems.at[6]))
    for load in small[:2] + loads[:1] + small[2:] + loads[1:]:
        load.start()

    barrier = pltpu.get_barrier_semaphore()

    @pl.loop(1, n, unroll=9)
    def _(d):
        pl.semaphore_signal(barrier, inc=1, device_id={"ep": (ep + d) % n}, device_id_type=MESH)

    @pl.loop(0, n, unroll=8)
    def _(d):
        there = {"ep": (ep + d) % n, "tp": across}
        pl.semaphore_signal(barrier, inc=1, device_id=there, device_id_type=MESH)

    for there in (mate, 3 - mate):
        pl.semaphore_signal(barrier, inc=1, device_id={"tp": there}, device_id_type=MESH)
    for load in small[:2] + loads[:1]:
        load.wait()
    rows = xin[...].astype(F)
    normed = (rows * lax.rsqrt(jnp.mean(rows * rows, axis=1, keepdims=True) + NORM_EPS) * xgain_ref[...]).astype(B)
    first, second = places(routes_ref, n)
    marks = jnp.where(first | second, 1.0, 0.0).astype(B)
    r, c, same = consts()
    for b in range(4):
        out_buf[16 * b : 16 * b + 16] = (
            dg(marks[128 * b : 128 * b + 128], normed, NN).reshape(16, 8, -1).astype(B)
        )

    pl.semaphore_wait(barrier, 2 * n + 1)

    pieces = ((gate_hbm, g_buf), (up_hbm, u_buf), (down_hbm, d_buf))
    sibling = {"ep": ep + other}

    def put(src, i, slot, sem, where):
        remote(src, pieces[i][1].at[slot], ws.at[sem], wr.at[3 * slot + i], where).start()

    def land(i, slot):
        wait_bytes(pieces[i][1].at[slot], wr.at[3 * slot + i])

    half = d_buf.shape[1] // 2
    halves = (pl.ds(0, half), pl.ds(half, half))

    def last(src, h, sem, where):
        remote(src, d_buf.at[3, halves[h]], ws.at[sem], wr.at[(11, 16)[h]], where).start()

    def last_land(h):
        wait_bytes(d_buf.at[3, halves[h]], wr.at[(11, 16)[h]])

    def hop(i):
        @pl.when(prime)
        def _():
            land(i, 2)
            if i < 2:
                put(pieces[i][1].at[2], i, 3, 6 + i, {"tp": mate})
            else:
                for h in range(2):
                    last(d_buf.at[2, halves[h]], h, (8, 21)[h], {"tp": mate})
            put(pieces[i][1].at[2], i, 2, 9 + i, sibling)

    def share(i, slot):
        @pl.when(prime)
        def _():
            land(i, slot)
            put(pieces[i][1].at[slot], i, slot, 12 + 3 * (slot // 3) + i, sibling)

    def others_land(i, slot):
        @pl.when(jnp.logical_not(prime))
        def _():
            land(i, slot)

    @pl.when(prime)
    def _():
        for i, (src, dst) in enumerate(pieces):
            put(src, i, 1, i, {"tp": mate})
        for i, (src, dst) in enumerate(pieces):
            put(src, i, 0, 3 + i, sibling)
            pltpu.make_async_copy(src, dst.at[0], wr.at[i]).start()

    @pl.when(jnp.logical_not(prime))
    def _():
        for i, (src, dst) in enumerate(pieces):
            put(src, i, 2, i, {"tp": across})

    def dispatch(e):
        differ = (e % 2 + tp // 2) % 2
        there = {"ep": e + differ * (1 - 2 * (e % 2)), "tp": tp + differ * (3 - 2 * tp)}
        remote(out_buf.at[e], arr_buf.at[ep], s4.at[0], s4.at[1], there).start()

    @pl.loop(0, n // 2)
    def _(d):
        dispatch((ep + 2 * d + 1) % n)

    for load in small[2:] + loads[1:6]:
        load.wait()

    high, rest = split(shift_ref[...])
    middle, low = split(shift_ref[...] - high.astype(F))
    shifts = jnp.concatenate([high.astype(F), middle.astype(F), low.astype(F)], 0).astype(B)

    @pl.loop(0, 4)
    def _(p):
        lanes = pl.ds(pl.multiple_of(p * 128, 128), 128)
        head = lax.broadcasted_iota(jnp.int32, (24, 128), 0) % 8
        lane = lax.broadcasted_iota(jnp.int32, (24, 128), 1)
        shift = dg(shifts, (head == 2 * p + lane // 64).astype(F).astype(B), TN)
        a = [mix_in[i, :, lanes] for i in range(5)]
        rd, lc, whole, offset = local_scan(*a, base_ref[:, lanes], shift)
        rd_buf[:, lanes] = rd.astype(B)
        lc_buf[:, lanes] = lc
        r, c, same = consts()
        less = fold(whole - jnp.where(r == c, 1.0, 0.0), C)
        mb_buf[p] = jnp.concatenate([less, fold(offset, C)], 0).astype(B)

    def row_copy(d, slot):
        j = (m + d) % 8
        return remote(mb_buf.at[j // 2], row_buf.at[slot], s1.at[d], r1.at[slot], {"ep": z * 8 + j})

    for d in range(1, 8):
        row_copy(d, m).start()

    @pl.loop(1, n // 4)
    def _(d):
        dispatch((ep + 4 * d) % n)

    hop(0)
    row_buf[m] = mb_buf[x]
    for d in range(1, 8):
        row_copy(d, (m + d) % 8).wait_recv()
    eye = fold(jnp.where(r == c, 1.0, 0.0).astype(F), C)
    none = jnp.zeros((C, 128), F)
    running = jnp.concatenate([eye, none], 0)
    for j in range(8):
        exc_buf[j] = running
        step, offset = unpack(row_buf[j])
        if j == 0:
            running = jnp.concatenate([fold(step, C), offset], 0)
        else:
            running = dot3(running, step, NN) + jnp.concatenate([none, offset], 0)
    tz_buf[...] = (running - jnp.concatenate([eye, none], 0)).astype(B)

    def z_copy(d, slot):
        return remote(tz_buf, z_buf.at[slot], s2.at[d], r2.at[slot], {"ep": ((z + d) % 8) * 8 + m})

    for d in range(1, 8):
        z_copy(d, z).start()

    @pl.when(prime)
    def _():
        pltpu.make_async_copy(out_buf.at[ep], arr_buf.at[ep], s4.at[1]).start()

    @pl.when(jnp.logical_not(prime))
    def _():
        dispatch(ep)

    @pl.loop(0, n // 4)
    def _(d):
        dispatch((ep + 4 * d + 2) % n)

    hop(1)
    for i in range(3):
        share(i, 1)
    z_buf[z] = tz_buf[...]
    for d in range(1, 8):
        z_copy(d, (z + d) % 8).wait_recv()
    state = none
    for j in range(7):
        step, offset = unpack(z_buf[j])
        after = offset if j == 0 else dot3(state, step, NN) + offset
        state = jnp.where(j < z, after, state)
    for k in range(4):
        member = exc_buf[k * 2 + core]
        fin_buf[k] = (dot3(state, spread(member[:C]), NN) + member[C:]).astype(B)

    def fin_copy(d, slot):
        k = (x + d) % 4
        return remote(fin_buf.at[k], st_buf.at[slot], s3.at[d], r3.at[slot], {"ep": z * 8 + k * 2 + core})

    for d in range(1, 4):
        fin_copy(d, x).start()

    st_buf[x] = fin_buf[x]
    for d in range(1, 4):
        fin_copy(d, (x + d) % 4).wait_recv()

    loads[6].wait()
    ones = jnp.where(same, 1.0 / 64, 0.0).astype(B)
    for b in range(4):
        here = slice(128 * b, 128 * b + 128)
        parts = []
        for p in range(4):
            lanes = slice(p * 128, (p + 1) * 128)
            read = lc_buf[here, lanes] + dg(rd_buf[here, lanes], spread(st_buf[p]), NT)
            centred = read - head_sum(read, ones)
            variance = head_sum(centred * centred, ones)
            parts.append((centred * lax.rsqrt(variance + GROUP_EPS) * gain_ref[:, lanes]).astype(B))
        part_buf[b] = dg(jnp.concatenate(parts, 1), wout[...], NN).astype(B)

    hop(2)
    def rs_copy(d, slot):
        j = (tp + d) % 4
        return remote(part_buf.at[j], rs_buf.at[slot], ws.at[17 + d], wr.at[12 + slot], {"tp": j})

    def rs_to(j):
        return remote(part_buf.at[j], rs_buf.at[tp], ws.at[18 + (j - tp + 3) % 4], wr.at[12 + tp], {"tp": j})

    rs_to(across).start()
    share(0, 3)

    wait_bytes(arr_buf, s4.at[1])

    def hidden(s, b):
        given = arr_buf[pl.ds(16 * b, 16)].reshape(128, -1)
        gate = dg(given, g_buf[s], NN)
        up = dg(given, u_buf[s], NN)
        return (gate / (1.0 + jnp.exp(-gate)) * up).astype(B)

    def units(s, b):
        return dg(hidden(s, b), d_buf[s], NN)

    def rows_of(b):
        return pl.ds(pl.multiple_of(b * 128, 128), 128)

    for i in range(3):
        land(i, 0)

    @pl.loop(0, 4)
    def _(b):
        acc[rows_of(b), :] = units(0, b)

    def add_slot(slot):
        for i in range(3):
            others_land(i, slot)

        @pl.loop(0, 4)
        def _(b):
            acc[rows_of(b), :] += units(slot, b)

    add_slot(1)
    share(1, 3)
    add_slot(2)
    for i in range(2):
        others_land(i, 3)

    @pl.loop(0, 4)
    def _(b):
        hid_buf[rows_of(b), :] = hidden(3, b)

    for h in range(2):
        last_land(h)

        @pl.when(prime)
        def _():
            last(d_buf.at[3, halves[h]], h, (17, 22)[h], sibling)

    rs_to(mate).start()
    rs_to(3 - mate).start()

    for offsets in ORDER:
        two = [(z + o) % 8 for o in offsets]
        block = [pl.ds(pl.multiple_of(64 * there, 64), 64) for there in two]
        low_part = dg(jnp.concatenate([hid_buf[b, :] for b in block], 0), d_buf[3], NN)
        for k, (there, b) in enumerate(zip(two, block)):
            full = acc[b, :] + low_part[64 * k : 64 * k + 64]
            res_buf[pl.ds(8 * there, 8)] = full.reshape(8, 8, -1).astype(B)

        @pl.loop(0, 16)
        def _(k):
            there = 8 * ((z + offsets[0] + (k % 2) * (offsets[1] - offsets[0])) % 8) + (m + k // 2) % 8

            @pl.when(jnp.logical_or(there != ep, jnp.logical_not(prime)))
            def _():
                where = {"ep": there, "tp": client}
                remote(res_buf.at[there], ret_buf.at[serves], misc.at[0], misc.at[1], where).start()

    @pl.when(prime)
    def _():
        pltpu.make_async_copy(res_buf.at[ep], ret_buf.at[ep], misc.at[1]).start()

    total = part_buf[tp].astype(F)
    for d in range(1, 4):
        rs_copy(d, (tp + d) % 4).wait_recv()
        total += rs_buf[(tp + d) % 4].astype(F)
    xin[...] = total.astype(B)
    leave = [pltpu.make_async_copy(xin, mixer_ref, in_sems.at[0])]
    leave[0].start()

    wait_bytes(ret_buf, misc.at[1])
    for d in range(1, 8):
        row_copy(d, m).wait_send()
        z_copy(d, z).wait_send()
    for d in range(1, 4):
        fin_copy(d, x).wait_send()
        rs_copy(d, tp).wait_send()

    def sent(count, rows_sent):
        for k in range(count):
            if k not in (8, 17):
                wait_bytes(pieces[k % 3][1].at[0], ws.at[k])
            else:
                for sem in (k, 21 + k // 17):
                    wait_bytes(d_buf.at[0, halves[0]], ws.at[sem])
        wait_bytes(out_buf.at[pl.ds(0, rows_sent)], s4.at[0])
        wait_bytes(res_buf.at[pl.ds(0, rows_sent)], misc.at[0])

    @pl.when(prime)
    def _():
        sent(18, n - 1)

    @pl.when(jnp.logical_not(prime))
    def _():
        sent(3, n)
    for copy in leave:
        copy.wait()


def finish_kernel(mixed, returned, routes_hbm, rw_hbm, mixer_ref, expert_ref, routes_ref, rw_ref, rows, mix, out, loaded, stored):
    count, width = rows.shape[0], rows.shape[2]
    parts = [pl.ds(width // 4 * k, width // 4) for k in range(4)]
    loads = [pltpu.make_async_copy(returned.at[:, :, p], rows.at[:, :, p], loaded.at[k]) for k, p in enumerate(parts)]
    loads.append(pltpu.make_async_copy(mixed, mix, loaded.at[4]))
    small = [
        pltpu.make_async_copy(routes_hbm, routes_ref, loaded.at[5]), pltpu.make_async_copy(rw_hbm, rw_ref, loaded.at[6])
    ]
    for load in small + loads:
        load.start()
    for load in small:
        load.wait()
    first, second = places(routes_ref, count)
    hi, lo = split(jnp.where(first, rw_ref[0:1, :], 0.0) + jnp.where(second, rw_ref[1:2, :], 0.0))
    stores = []
    for k, p in enumerate(parts):
        loads[k].wait()
        given = rows[:, :, p].reshape(count * 8, -1)
        out[:, p] = (dg(hi, given, TN) + dg(lo, given, TN)).astype(B)
        stores.append(pltpu.make_async_copy(out.at[:, p], expert_ref.at[:, p], stored.at[k]))
        stores[k].start()
        if k == 1:
            loads[4].wait()
            leave = pltpu.make_async_copy(mix, mixer_ref, stored.at[4])
            leave.start()
    stores.append(leave)
    for store in stores:
        store.wait()


def on_device(
    receptance, key_rows, value_rows, decay_input, learn_input, decay_base, decay_shift, channel_gain,
    out_weight, expert_input, expert_gain, routes, route_weight, gate_weight, up_weight, down_weight,
):
    t, width = expert_input.shape
    rows, channels = receptance.shape
    depth, units = gate_weight.shape[1:]
    anywhere = pl.BlockSpec(memory_space=pltpu.HBM)
    dma = pltpu.SemaphoreType.DMA
    V = pltpu.VMEM
    both = jax.ShapeDtypeStruct((t, width), B)
    mixed, returned = pl.pallas_call(
        kernel,
        in_specs=[anywhere] * 15,
        out_specs=[anywhere, anywhere],
        out_shape=[both, jax.ShapeDtypeStruct((64, 8, width), B)],
        scratch_shapes=[
            V((1, channels), F), V((8, rows), F), V((1, channels), F), V((1, width), F), V((2, t), jnp.int32),
            V((5, rows, channels), B), V((channels, width), B), V((t, width), B),
            V((4, depth, units), B), V((4, depth, units), B), V((4, units, width), B),
            V((rows, channels), B), V((rows, channels), F),
            V((4, 128, 128), B), V((8, 128, 128), B), V((8, 128, 128), F), V((128, 128), B), V((8, 128, 128), B),
            V((4, C, 128), B), V((4, C, 128), B),
            V((64, 8, width), B), V((64, 8, width), B), V((512, width), F), V((512, units), B),
            V((64, 8, width), B), V((4, t, width), B), V((4, t, width), B),
            dma((12,)), dma((23,)), dma((17,)), dma((8,)), dma((8,)), dma((8,)), dma((8,)), dma((4,)), dma((4,)),
            dma((2,)), dma((2,)),
        ],
        compiler_params=pltpu.CompilerParams(
            collective_id=0, has_side_effects=True, vmem_limit_bytes=60 * 1024 * 1024
        ),
        name="step",
    )(
        receptance, key_rows, value_rows, decay_input, learn_input, out_weight, expert_input,
        gate_weight[0], up_weight[0], down_weight[0],
        decay_base.reshape(1, channels), decay_shift.T, channel_gain.reshape(1, channels), expert_gain.reshape(1, width),
        routes.T,
    )
    return pl.pallas_call(
        finish_kernel,
        in_specs=[anywhere] * 4,
        out_specs=[anywhere, anywhere],
        out_shape=[both, both],
        scratch_shapes=[
            V((2, t), jnp.int32), V((2, t), F), V((64, 8, width), B), V((t, width), B), V((t, width), B), dma((7,)), dma((5,)),
        ],
        name="finish",
    )(mixed, returned, routes.T, route_weight.T)


def solution(mesh):
    both = P(("ep", "tp"), None)
    placed = (
        P("ep", "tp"), P("ep", "tp"), P("ep", "tp"), P("ep", "tp"), P("ep", "tp"), P("tp"), P("ep", "tp"), P("tp"),
        P("tp", None), both, P(), both, both, P("ep", None, "tp"), P("ep", None, "tp"), P("ep", "tp", None),
    )
    return jax.shard_map(on_device, mesh=mesh, in_specs=placed, out_specs=(both, both), check_vma=False)
```

```python
import functools

import jax
import jax.numpy as jnp
from jax import lax
from jax.experimental import pallas as pl
from jax.experimental.pallas import tpu as pltpu
from jax.sharding import PartitionSpec as P


MESH = pl.DeviceIdType.MESH
NORM_EPS = 1e-06
GROUP_EPS = 0.00064
F=jnp.float32; B=jnp.bfloat16
C=64
NT=(((1,),(1,)),((),())); NN=(((1,),(0,)),((),())); TN=(((0,),(0,)),((),()))
def dg(a,b,dims): return lax.dot_general(a,b,dims,preferred_element_type=F)
def split(x):
    hi=x.astype(B); return hi,(x-hi.astype(F)).astype(B)
def dot3(a,b,dims):
    ah,al=split(a); bh,bl=split(b)
    return dg(ah,bh,dims)+(dg(ah,bl,dims)+dg(al,bh,dims))
def fold(x,n): return x[:n]+x[n:]
def consts():
    r=lax.broadcasted_iota(jnp.int32,(128,128),0); c=lax.broadcasted_iota(jnp.int32,(128,128),1)
    same=(r//64)==(c//64)
    return r,c,same
def pre_stage(key,dec,learn,base,shift):
    r,c,same=consts()
    ones=same.astype(B)
    kf=key.astype(F)
    hi,lo=split(kf*kf)
    ss=dg(hi,ones,NN)+dg(lo,ones,NN)
    unit=kf*lax.rsqrt(ss+1e-6)
    pre=dec.astype(F)+base+shift
    ld=-0.6065306597126334/(1.0+jnp.exp(-pre))
    rem=unit/(1.0+jnp.exp(-learn.astype(F)))
    return kf,unit,ld,rem
def chunk_cum(ld):
    r,c,same=consts()
    tri=(same&(r>=c)).astype(B)
    outs=[]
    for i in range(ld.shape[0]//128):
        hi,lo=split(ld[i*128:(i+1)*128])
        outs.append(dg(tri,hi,NN)+dg(tri,lo,NN))
    return jnp.concatenate(outs,0)
def chunk(rec,kf,vb,unit,rem,ld,cum):
    r,c,same=consts()
    lane=lax.broadcasted_iota(jnp.int32,(C,128),1)
    m0=lane<64
    mid=cum[C//2-1:C//2]; end=cum[C-1:C]
    rel=cum-mid
    Q=rec*jnp.exp(rel); P=unit*jnp.exp(rel-ld)
    sh=jnp.exp(-rel)
    BR=(rem*sh).astype(B); BK=(kf*sh).astype(B)
    Qb=Q.astype(B); Pb=P.astype(B)
    z=jnp.zeros((C,128),B)
    ex=lambda x: jnp.concatenate([jnp.where(m0,x,z),jnp.where(m0,z,x)],0)
    Pe=ex(Pb)
    lhs=jnp.concatenate([Pe,ex(Qb)],0)
    sR=dg(lhs,jnp.concatenate([BR,BR],0),NT)
    sK=dg(lhs,jnp.concatenate([BK,BK],0),NT)
    yield None
    strict=same&(r>c); incl=same&(r>=c)
    zf=jnp.zeros((128,128),F)
    A=jnp.where(strict,sR[:128],zf).astype(B)
    PK=jnp.where(strict,sK[:128],zf).astype(B)
    QR=jnp.where(incl,sR[128:],zf).astype(B)
    QK=jnp.where(incl,sK[128:],zf).astype(B)
    zb=jnp.zeros((128,128),B)
    x=r^c
    lm=lambda m: (x>=m)&(x<2*m)
    D=jnp.where(r==c,1.0,0.0).astype(B)-jnp.where(lm(1),A,zb)
    m=2
    while m<C:
        E=dg(jnp.where(lm(m),A,zb),D,NN).astype(B)
        yield None
        D=D-dg(D,E,NN).astype(B)
        yield None
        m*=2
    Ve=ex(vb)
    kv=dg(jnp.concatenate([PK,QK],0),Ve,NN)
    yield None
    X=dg(D,jnp.concatenate([Pe,kv[:128].astype(B)],1),NN)
    Xb=X.astype(B)
    yield None
    qx=dg(QR,Xb,NN)
    yield None
    em=jnp.exp(mid); et=jnp.exp(end-mid)
    reader=(Q-fold(qx[:,:128],C))*em
    local=fold(kv[128:],C)-fold(qx[:,128:],C)
    X0=fold(Xb[:,:128],C); L=fold(Xb[:,128:],C)
    tx=dg(X0,BR,TN)
    yield None
    eye=jnp.where(r==c,1.0,0.0).astype(F)
    emT=jnp.sum(jnp.where(r==c,jnp.broadcast_to(em,(128,128)),zf),1,keepdims=True)
    T=jnp.where(same,(eye-tx)*emT*et,zf)
    off=dg(jnp.concatenate([vb,-L],0),jnp.concatenate([BK,BR],0),TN)
    off=jnp.where(same,off*et,zf)
    yield reader,local,T,off
def local_scan(rec,key,val,dec,learn,base,shift):
    n=key.shape[0]//C
    kf,unit,ld,rem=pre_stage(key,dec,learn,base,shift)
    cum=chunk_cum(ld)
    outs=[]
    for i in range(n):
        s=slice(i*C,(i+1)*C)
        outs.append(chunk(rec[s].astype(F),kf[s],val[s],unit[s],rem[s],ld[s],cum[s]))
    while True:
        now=[next(o) for o in outs]
        if now[0] is not None: break
    outs=now
    r,c,same=consts()
    PB=None
    rd=[];lc=[]
    for i in range(n):
        reader,local,T,off=outs[i]
        if PB is None:
            rd.append(reader); lc.append(local)
            PB=jnp.concatenate([T,off],0)
        else:
            ph,pl_=split(PB)
            rh=reader.astype(B)
            q=dg(rh,ph,NT)
            rd.append(q[:,:128]); lc.append(local+q[:,128:])
            PB=dot3(PB,T,NN)+jnp.concatenate([jnp.zeros_like(off),off],0)
    return jnp.concatenate(rd,0),jnp.concatenate(lc,0),PB[:128],PB[128:]


def spread(compact):
    lane = lax.broadcasted_iota(jnp.int32, compact.shape, 1)
    nil = jnp.zeros_like(compact)
    return jnp.concatenate([jnp.where(lane < 64, compact, nil), jnp.where(lane < 64, nil, compact)], 0)


def unpack(message):
    r, c, same = consts()
    eye = jnp.where(r == c, 1.0, 0.0).astype(F)
    wide = message.astype(F)
    return spread(wide[:C]) + eye, wide[C:]


def head_sum(x, ones):
    hi, lo = split(x)
    return dg(hi, ones, NN) + dg(lo, ones, NN)


def places(routes_ref, experts):
    r0, r1 = routes_ref[0:1, :], routes_ref[1:2, :]
    r, c, same = consts()
    hits = ((r == r0) | (r == r1)).astype(F).astype(B)
    earlier = dg(hits, (r < c).astype(F).astype(B), NN)
    t0 = r0.astype(F) * 8.0 + jnp.sum(jnp.where(r == r0, earlier, 0.0), 0, keepdims=True)
    t1 = r1.astype(F) * 8.0 + jnp.sum(jnp.where(r == r1, earlier, 0.0), 0, keepdims=True)
    place = lax.broadcasted_iota(jnp.int32, (experts * 8, 128), 0).astype(F)
    return place == t0, place == t1


def remote(src, dst, send, recv, where):
    return pltpu.make_async_remote_copy(
        src_ref=src, dst_ref=dst, send_sem=send, recv_sem=recv, device_id=where, device_id_type=MESH
    )


def wait_bytes(ref, sem):
    pltpu.make_async_copy(ref, ref, sem).wait()


ORDER = ((1, 7), (2, 6), (3, 5), (0, 4))


def kernel(
    rec_hbm, key_hbm, val_hbm, dec_hbm, learn_hbm, wout_hbm, x_hbm, gate_hbm, up_hbm, down_hbm,
    base_hbm, shift_hbm, gain_hbm, xgain_hbm, routes_hbm,
    mixer_ref, ret_buf,
    base_ref, shift_ref, gain_ref, xgain_ref, routes_ref,
    mix_in, wout, xin, g_buf, u_buf, d_buf, rd_buf, lc_buf, mb_buf, row_buf, exc_buf, tz_buf, z_buf, fin_buf, st_buf,
    out_buf, arr_buf, acc, hid_buf, res_buf, part_buf, rs_buf,
    in_sems, ws, wr, s1, r1, s2, r2, s3, r3, s4, misc,
):
    ep, tp = lax.axis_index("ep"), lax.axis_index("tp")
    z, m = ep // 8, ep % 8
    x, core = m // 2, m % 2
    n = 64
    mate, across = tp + 1 - 2 * (tp % 2), 3 - tp
    other = 1 - 2 * core
    prime = core == tp // 2
    client = jnp.where(prime, tp, across)
    serves = jnp.where(prime, ep, ep + other)

    smalls = ((routes_hbm, routes_ref), (xgain_hbm, xgain_ref), (base_hbm, base_ref), (shift_hbm, shift_ref), (gain_hbm, gain_ref))
    small = [pltpu.make_async_copy(src, dst, in_sems.at[7 + i]) for i, (src, dst) in enumerate(smalls)]
    loads = [pltpu.make_async_copy(x_hbm, xin, in_sems.at[0])]
    for i, src in enumerate((rec_hbm, key_hbm, val_hbm, dec_hbm, learn_hbm)):
        loads.append(pltpu.make_async_copy(src, mix_in.at[i], in_sems.at[i + 1]))
    loads.append(pltpu.make_async_copy(wout_hbm, wout, in_sems.at[6]))
    for load in small[:2] + loads[:1] + small[2:] + loads[1:]:
        load.start()

    barrier = pltpu.get_barrier_semaphore()

    def greet(there):
        pl.semaphore_signal(barrier, inc=1, device_id=there, device_id_type=MESH)

    for there in (mate, 3 - mate):
        greet({"tp": there})

    @pl.loop(0, n // 2, unroll=8)
    def _(d):
        greet({"ep": (ep + 2 * d + 1) % n})
        greet({"ep": (ep + 2 * d) % n, "tp": across})

    @pl.when(prime)
    def _():
        @pl.loop(1, n // 2)
        def _(d):
            greet({"ep": (ep + 2 * d) % n})

        pl.semaphore_wait(barrier, 2 + n + n // 2 - 1)

    @pl.when(jnp.logical_not(prime))
    def _():
        @pl.loop(0, n // 2, unroll=8)
        def _(d):
            greet({"ep": (ep + 2 * d + 1) % n, "tp": across})

        for d in range(1, 4):
            greet({"ep": z * 8 + (m + 2 * d) % 8})
        for d in range(1, 8):
            greet({"ep": ((z + d) % 8) * 8 + m})
        pl.semaphore_wait(barrier, 2 + n + n // 2 + 10)

    pieces = ((gate_hbm, g_buf), (up_hbm, u_buf), (down_hbm, d_buf))
    sibling = {"ep": ep + other}

    def put(src, i, slot, sem, where):
        remote(src, pieces[i][1].at[slot], ws.at[sem], wr.at[3 * slot + i], where).start()

    def land(i, slot):
        wait_bytes(pieces[i][1].at[slot], wr.at[3 * slot + i])

    half = d_buf.shape[1] // 2
    halves = (pl.ds(0, half), pl.ds(half, half))

    def last(src, h, sem, where):
        remote(src, d_buf.at[3, halves[h]], ws.at[sem], wr.at[(11, 16)[h]], where).start()

    def last_land(h):
        wait_bytes(d_buf.at[3, halves[h]], wr.at[(11, 16)[h]])

    def hop(i):
        @pl.when(prime)
        def _():
            land(i, 2)
            if i < 2:
                put(pieces[i][1].at[2], i, 3, 6 + i, {"tp": mate})
            else:
                for h in range(2):
                    last(d_buf.at[2, halves[h]], h, (8, 21)[h], {"tp": mate})
            put(pieces[i][1].at[2], i, 2, 9 + i, sibling)

    def share(i, slot):
        @pl.when(prime)
        def _():
            land(i, slot)
            put(pieces[i][1].at[slot], i, slot, 12 + 3 * (slot // 3) + i, sibling)

    def others_land(i, slot):
        @pl.when(jnp.logical_not(prime))
        def _():
            land(i, slot)

    @pl.when(prime)
    def _():
        for i, (src, dst) in enumerate(pieces):
            put(src, i, 1, i, {"tp": mate})
        for i, (src, dst) in enumerate(pieces):
            put(src, i, 0, 3 + i, sibling)
            pltpu.make_async_copy(src, dst.at[0], wr.at[i]).start()

    @pl.when(jnp.logical_not(prime))
    def _():
        for i, (src, dst) in enumerate(pieces):
            put(src, i, 2, i, {"tp": across})

    for load in small[:2] + loads[:1]:
        load.wait()
    rows = xin[...].astype(F)
    normed = (rows * lax.rsqrt(jnp.mean(rows * rows, axis=1, keepdims=True) + NORM_EPS) * xgain_ref[...]).astype(B)
    first, second = places(routes_ref, n)
    marks = jnp.where(first | second, 1.0, 0.0).astype(B)
    r, c, same = consts()
    for b in range(4):
        out_buf[16 * b : 16 * b + 16] = (
            dg(marks[128 * b : 128 * b + 128], normed, NN).reshape(16, 8, -1).astype(B)
        )

    def dispatch(e):
        differ = (e % 2 + tp // 2) % 2
        there = {"ep": e + differ * (1 - 2 * (e % 2)), "tp": tp + differ * (3 - 2 * tp)}
        remote(out_buf.at[e], arr_buf.at[ep], s4.at[0], s4.at[1], there).start()

    odd = jnp.where(prime, 0, 1)

    @pl.loop(0, n // 2)
    def _(d):
        @pl.when(d + odd > 0)
        def _():
            dispatch((ep + 2 * d + odd) % n)

    @pl.when(prime)
    def _():
        pltpu.make_async_copy(out_buf.at[ep], arr_buf.at[ep], s4.at[1]).start()

    for load in small[2:] + loads[1:6]:
        load.wait()

    high, rest = split(shift_ref[...])
    middle, low = split(shift_ref[...] - high.astype(F))
    shifts = jnp.concatenate([high.astype(F), middle.astype(F), low.astype(F)], 0).astype(B)

    @pl.loop(0, 4)
    def _(p):
        lanes = pl.ds(pl.multiple_of(p * 128, 128), 128)
        head = lax.broadcasted_iota(jnp.int32, (24, 128), 0) % 8
        lane = lax.broadcasted_iota(jnp.int32, (24, 128), 1)
        shift = dg(shifts, (head == 2 * p + lane // 64).astype(F).astype(B), TN)
        a = [mix_in[i, :, lanes] for i in range(5)]
        rd, lc, whole, offset = local_scan(*a, base_ref[:, lanes], shift)
        rd_buf[:, lanes] = rd.astype(B)
        lc_buf[:, lanes] = lc
        r, c, same = consts()
        less = fold(whole - jnp.where(r == c, 1.0, 0.0), C)
        mb_buf[p] = jnp.concatenate([less, fold(offset, C)], 0).astype(B)

    def row_copy(d, slot):
        j = (m + d) % 8
        return remote(mb_buf.at[j // 2], row_buf.at[slot], s1.at[d], r1.at[slot], {"ep": z * 8 + j})

    for d in range(1, 8):
        row_copy(d, m).start()

    @pl.loop(0, n // 4)
    def _(d):
        dispatch((ep + 4 * d + 1 - odd) % n)

    hop(0)
    row_buf[m] = mb_buf[x]
    for d in range(1, 8):
        row_copy(d, (m + d) % 8).wait_recv()
    eye = fold(jnp.where(r == c, 1.0, 0.0).astype(F), C)
    none = jnp.zeros((C, 128), F)
    running = jnp.concatenate([eye, none], 0)
    for j in range(8):
        exc_buf[j] = running
        step, offset = unpack(row_buf[j])
        if j == 0:
            running = jnp.concatenate([fold(step, C), offset], 0)
        else:
            running = dot3(running, step, NN) + jnp.concatenate([none, offset], 0)
    tz_buf[...] = (running - jnp.concatenate([eye, none], 0)).astype(B)

    def z_copy(d, slot):
        return remote(tz_buf, z_buf.at[slot], s2.at[d], r2.at[slot], {"ep": ((z + d) % 8) * 8 + m})

    for d in range(1, 8):
        z_copy(d, z).start()

    @pl.loop(0, n // 4)
    def _(d):
        dispatch((ep + 4 * d + 3 - odd) % n)

    hop(1)
    for i in range(3):
        share(i, 1)
    z_buf[z] = tz_buf[...]
    for d in range(1, 8):
        z_copy(d, (z + d) % 8).wait_recv()
    state = none
    for j in range(7):
        step, offset = unpack(z_buf[j])
        after = offset if j == 0 else dot3(state, step, NN) + offset
        state = jnp.where(j < z, after, state)
    for k in range(4):
        member = exc_buf[k * 2 + core]
        fin_buf[k] = (dot3(state, spread(member[:C]), NN) + member[C:]).astype(B)

    def fin_copy(d, slot):
        k = (x + d) % 4
        return remote(fin_buf.at[k], st_buf.at[slot], s3.at[d], r3.at[slot], {"ep": z * 8 + k * 2 + core})

    for d in range(1, 4):
        fin_copy(d, x).start()

    st_buf[x] = fin_buf[x]
    for d in range(1, 4):
        fin_copy(d, (x + d) % 4).wait_recv()

    loads[6].wait()
    ones = jnp.where(same, 1.0 / 64, 0.0).astype(B)
    for b in range(4):
        here = slice(128 * b, 128 * b + 128)
        parts = []
        for p in range(4):
            lanes = slice(p * 128, (p + 1) * 128)
            read = lc_buf[here, lanes] + dg(rd_buf[here, lanes], spread(st_buf[p]), NT)
            centred = read - head_sum(read, ones)
            variance = head_sum(centred * centred, ones)
            parts.append((centred * lax.rsqrt(variance + GROUP_EPS) * gain_ref[:, lanes]).astype(B))
        part_buf[b] = dg(jnp.concatenate(parts, 1), wout[...], NN).astype(B)

    hop(2)
    def rs_copy(d, slot):
        j = (tp + d) % 4
        return remote(part_buf.at[j], rs_buf.at[slot], ws.at[17 + d], wr.at[12 + slot], {"tp": j})

    def rs_to(j):
        return remote(part_buf.at[j], rs_buf.at[tp], ws.at[18 + (j - tp + 3) % 4], wr.at[12 + tp], {"tp": j})

    rs_to(across).start()
    share(0, 3)

    wait_bytes(arr_buf, s4.at[1])

    def hidden(s, b):
        given = arr_buf[pl.ds(16 * b, 16)].reshape(128, -1)
        gate = dg(given, g_buf[s], NN)
        up = dg(given, u_buf[s], NN)
        return (gate / (1.0 + jnp.exp(-gate)) * up).astype(B)

    def units(s, b):
        return dg(hidden(s, b), d_buf[s], NN)

    def rows_of(b):
        return pl.ds(pl.multiple_of(b * 128, 128), 128)

    for i in range(3):
        land(i, 0)

    @pl.loop(0, 4)
    def _(b):
        acc[rows_of(b), :] = units(0, b)

    def add_slot(slot):
        for i in range(3):
            others_land(i, slot)

        @pl.loop(0, 4)
        def _(b):
            acc[rows_of(b), :] += units(slot, b)

    add_slot(1)
    share(1, 3)
    add_slot(2)
    for i in range(2):
        others_land(i, 3)

    @pl.loop(0, 4)
    def _(b):
        hid_buf[rows_of(b), :] = hidden(3, b)

    for h in range(2):
        last_land(h)

        @pl.when(prime)
        def _():
            last(d_buf.at[3, halves[h]], h, (17, 22)[h], sibling)

    rs_to(mate).start()
    rs_to(3 - mate).start()

    for offsets in ORDER:
        two = [(z + o) % 8 for o in offsets]
        block = [pl.ds(pl.multiple_of(64 * there, 64), 64) for there in two]
        low_part = dg(jnp.concatenate([hid_buf[b, :] for b in block], 0), d_buf[3], NN)
        for k, (there, b) in enumerate(zip(two, block)):
            full = acc[b, :] + low_part[64 * k : 64 * k + 64]
            res_buf[pl.ds(8 * there, 8)] = full.reshape(8, 8, -1).astype(B)

        @pl.loop(0, 16)
        def _(k):
            there = 8 * ((z + offsets[0] + (k % 2) * (offsets[1] - offsets[0])) % 8) + (m + k // 2) % 8

            @pl.when(jnp.logical_or(there != ep, jnp.logical_not(prime)))
            def _():
                where = {"ep": there, "tp": client}
                remote(res_buf.at[there], ret_buf.at[serves], misc.at[0], misc.at[1], where).start()

    @pl.when(prime)
    def _():
        pltpu.make_async_copy(res_buf.at[ep], ret_buf.at[ep], misc.at[1]).start()

    total = part_buf[tp].astype(F)
    for d in range(1, 4):
        rs_copy(d, (tp + d) % 4).wait_recv()
        total += rs_buf[(tp + d) % 4].astype(F)
    xin[...] = total.astype(B)
    leave = [pltpu.make_async_copy(xin, mixer_ref, in_sems.at[0])]
    leave[0].start()

    wait_bytes(ret_buf, misc.at[1])
    for d in range(1, 8):
        row_copy(d, m).wait_send()
        z_copy(d, z).wait_send()
    for d in range(1, 4):
        fin_copy(d, x).wait_send()
        rs_copy(d, tp).wait_send()

    def sent(count, rows_sent):
        for k in range(count):
            if k not in (8, 17):
                wait_bytes(pieces[k % 3][1].at[0], ws.at[k])
            else:
                for sem in (k, 21 + k // 17):
                    wait_bytes(d_buf.at[0, halves[0]], ws.at[sem])
        wait_bytes(out_buf.at[pl.ds(0, rows_sent)], s4.at[0])
        wait_bytes(res_buf.at[pl.ds(0, rows_sent)], misc.at[0])

    @pl.when(prime)
    def _():
        sent(18, n - 1)

    @pl.when(jnp.logical_not(prime))
    def _():
        sent(3, n)
    for copy in leave:
        copy.wait()


def finish_kernel(mixed, returned, routes_hbm, rw_hbm, mixer_ref, expert_ref, routes_ref, rw_ref, rows, mix, out, loaded, stored):
    count, width = rows.shape[0], rows.shape[2]
    parts = [pl.ds(width // 4 * k, width // 4) for k in range(4)]
    loads = [pltpu.make_async_copy(returned.at[:, :, p], rows.at[:, :, p], loaded.at[k]) for k, p in enumerate(parts)]
    loads.append(pltpu.make_async_copy(mixed, mix, loaded.at[4]))
    small = [
        pltpu.make_async_copy(routes_hbm, routes_ref, loaded.at[5]), pltpu.make_async_copy(rw_hbm, rw_ref, loaded.at[6])
    ]
    for load in small + loads:
        load.start()
    for load in small:
        load.wait()
    first, second = places(routes_ref, count)
    hi, lo = split(jnp.where(first, rw_ref[0:1, :], 0.0) + jnp.where(second, rw_ref[1:2, :], 0.0))
    stores = []
    for k, p in enumerate(parts):
        loads[k].wait()
        given = rows[:, :, p].reshape(count * 8, -1)
        out[:, p] = (dg(hi, given, TN) + dg(lo, given, TN)).astype(B)
        stores.append(pltpu.make_async_copy(out.at[:, p], expert_ref.at[:, p], stored.at[k]))
        stores[k].start()
        if k == 1:
            loads[4].wait()
            leave = pltpu.make_async_copy(mix, mixer_ref, stored.at[4])
            leave.start()
    stores.append(leave)
    for store in stores:
        store.wait()


def on_device(
    receptance, key_rows, value_rows, decay_input, learn_input, decay_base, decay_shift, channel_gain,
    out_weight, expert_input, expert_gain, routes, route_weight, gate_weight, up_weight, down_weight,
):
    t, width = expert_input.shape
    rows, channels = receptance.shape
    depth, units = gate_weight.shape[1:]
    anywhere = pl.BlockSpec(memory_space=pltpu.HBM)
    dma = pltpu.SemaphoreType.DMA
    V = pltpu.VMEM
    both = jax.ShapeDtypeStruct((t, width), B)
    mixed, returned = pl.pallas_call(
        kernel,
        in_specs=[anywhere] * 15,
        out_specs=[anywhere, anywhere],
        out_shape=[both, jax.ShapeDtypeStruct((64, 8, width), B)],
        scratch_shapes=[
            V((1, channels), F), V((8, rows), F), V((1, channels), F), V((1, width), F), V((2, t), jnp.int32),
            V((5, rows, channels), B), V((channels, width), B), V((t, width), B),
            V((4, depth, units), B), V((4, depth, units), B), V((4, units, width), B),
            V((rows, channels), B), V((rows, channels), F),
            V((4, 128, 128), B), V((8, 128, 128), B), V((8, 128, 128), F), V((128, 128), B), V((8, 128, 128), B),
            V((4, C, 128), B), V((4, C, 128), B),
            V((64, 8, width), B), V((64, 8, width), B), V((512, width), F), V((512, units), B),
            V((64, 8, width), B), V((4, t, width), B), V((4, t, width), B),
            dma((12,)), dma((23,)), dma((17,)), dma((8,)), dma((8,)), dma((8,)), dma((8,)), dma((4,)), dma((4,)),
            dma((2,)), dma((2,)),
        ],
        compiler_params=pltpu.CompilerParams(
            collective_id=0, has_side_effects=True, vmem_limit_bytes=60 * 1024 * 1024
        ),
        name="step",
    )(
        receptance, key_rows, value_rows, decay_input, learn_input, out_weight, expert_input,
        gate_weight[0], up_weight[0], down_weight[0],
        decay_base.reshape(1, channels), decay_shift.T, channel_gain.reshape(1, channels), expert_gain.reshape(1, width),
        routes.T,
    )
    return pl.pallas_call(
        finish_kernel,
        in_specs=[anywhere] * 4,
        out_specs=[anywhere, anywhere],
        out_shape=[both, both],
        scratch_shapes=[
            V((2, t), jnp.int32), V((2, t), F), V((64, 8, width), B), V((t, width), B), V((t, width), B), dma((7,)), dma((5,)),
        ],
        name="finish",
    )(mixed, returned, routes.T, route_weight.T)


def solution(mesh):
    both = P(("ep", "tp"), None)
    placed = (
        P("ep", "tp"), P("ep", "tp"), P("ep", "tp"), P("ep", "tp"), P("ep", "tp"), P("tp"), P("ep", "tp"), P("tp"),
        P("tp", None), both, P(), both, both, P("ep", None, "tp"), P("ep", None, "tp"), P("ep", "tp", None),
    )
    return jax.shard_map(on_device, mesh=mesh, in_specs=placed, out_specs=(both, both), check_vma=False)
```
